32 devices in a mesh: ra: 8 (over z, y), cb: 4 (over x, core).
Axes of the slice: x: 2, y: 2, z: 4, core: 2. Of those that a mesh axis runs over, the one named last changes fastest.
Arguments:
- tokens: bfloat16 [512, 4096], P(None, 'cb'), may hold values from -400 to 400
- norm_gain: bfloat16 [4096], P('cb'), may hold values from 0.099609375 to 1.8984375
- w_gate: bfloat16 [4096, 11264], P('cb', 'ra'), may hold values from -0.09375 to 0.09375
- w_up: bfloat16 [4096, 11264], P('cb', 'ra'), may hold values from -0.09375 to 0.09375
- w_down: bfloat16 [11264, 4096], P('ra', 'cb'), may hold values from -0.0546875 to 0.0546875
- out_gain: bfloat16 [4096], P('cb'), may hold values from 0.099609375 to 1.8984375
Outputs:
- normed_out: bfloat16 [512, 4096], P('ra', 'cb')
The draws below stay inside these ranges and needn't reach their ends.
All inputs are finite; a program needn't handle non-finite values.
Results may differ from the reference program's by a relative error of at most 0.0045.
Values sent between devices are 32-bit elements; how exact they have to be, the bound alone decides.
A program may use at most 64 MiB of HBM per device.

```python
import jax
import jax.numpy as jnp
from jax import lax

D = 4096
FF = 11264
TOKENS = 512


def draw_tokens(key, part):
    first, second, third = jax.random.split(jax.random.fold_in(key, 17), 3)
    rise = jnp.arange(D, dtype=jnp.float32) / D
    jitter = jax.random.uniform(second, (D,), jnp.float32)
    column_scale = jnp.exp(jnp.log(10.0) * (0.8 * rise + 0.2 * jitter))
    row_scale = jnp.exp(jnp.log(10.0) * jax.random.uniform(third, (TOKENS, 1), jnp.float32))
    base = jnp.clip(jax.random.normal(first, (TOKENS, D), jnp.float32), -4.0, 4.0)
    return (base * row_scale * column_scale[None, :]).astype(jnp.bfloat16)


def level_of(stream_key, dims, cuts, least, largest):
    gain, own = 1.0, jax.random.fold_in(stream_key, 6)
    for dim, parts in cuts:
        draws = jnp.exp(jax.random.uniform(jax.random.fold_in(own, dim), (parts,), jnp.float32, least / len(cuts), largest / len(cuts)))
        gain = gain * jnp.repeat(draws, dims[dim] // parts).reshape([-1 if axis == dim else 1 for axis in range(len(dims))])
    return gain


def scatter_about(rng, shape, deviation, most, shards=(), held_as=jnp.bfloat16):
    loudness = level_of(rng, shape, shards, -0.22, 0.18) if shards else 1.0
    drawn = jax.random.normal(rng, shape, jnp.float32) * deviation * loudness
    return jnp.minimum(jnp.maximum(drawn, -most), most).astype(held_as)


def setup_inputs(seed: int = 0) -> dict:
    keys = jax.random.split(jax.random.key(seed), 7)
    return {
        "tokens": draw_tokens(jax.random.fold_in(keys[6], 71), 0),
        "norm_gain": jnp.clip(1.0 + 0.18 * jax.random.normal(keys[1], (D,), jnp.float32), 0.099609375, 1.8984375).astype(jnp.bfloat16),
        "w_gate": scatter_about(keys[2], (D, FF), D ** -0.5, 0.09375, ((0, 4), (1, 8))),
        "w_up": scatter_about(keys[3], (D, FF), D ** -0.5, 0.09375, ((0, 4), (1, 8))),
        "w_down": scatter_about(keys[4], (FF, D), FF ** -0.5, 0.0546875, ((0, 8), (1, 4))),
        "out_gain": jnp.clip(1.0 + 0.18 * jax.random.normal(keys[5], (D,), jnp.float32), 0.099609375, 1.8984375).astype(jnp.bfloat16),
    }


def reference(tokens, norm_gain, w_gate, w_up, w_down, out_gain):
    eps = 1e-06
    xfloat = tokens.astype(jnp.float32)
    inv_in = lax.rsqrt(lax.optimization_barrier(jnp.mean(xfloat * xfloat, axis=1, keepdims=True)) + eps)
    scaled = (xfloat * norm_gain.astype(jnp.float32)).astype(jnp.bfloat16)
    gate = jnp.dot(scaled, w_gate, preferred_element_type=jnp.float32) * inv_in
    up = jnp.dot(scaled, w_up, preferred_element_type=jnp.float32) * inv_in
    hidden = (jax.nn.silu(gate) * up).astype(jnp.bfloat16)
    down = jnp.dot(hidden, w_down, preferred_element_type=jnp.float32)
    mixed = 0.1 * xfloat + down
    inv_out = lax.rsqrt(lax.optimization_barrier(jnp.mean(mixed * mixed, axis=1, keepdims=True)) + eps)
    return (mixed * inv_out * out_gain.astype(jnp.float32)).astype(jnp.bfloat16)
```

```python
import functools

import jax
import jax.numpy as jnp
from jax import lax
from jax.experimental import pallas as pl
from jax.experimental.pallas import tpu as pltpu
from jax.sharding import PartitionSpec as P

EPS = 1e-06
LANES = 128
TILE = 256
PIECES = 3
SLICES = 2
SHARES = (1, 2, 2, 1, 1, 1)
UNITS = sum(SHARES)
VMEM_BYTES = 63 * 1024 * 1024 - 64 * 1024


def plain_body(width, tokens, norm_gain, w_gate, w_up, w_down, out_gain):
    xfloat = tokens.astype(jnp.float32)
    local_sq = jnp.sum(xfloat * xfloat, axis=1)
    scaled = (xfloat * norm_gain.astype(jnp.float32)).astype(jnp.bfloat16)
    gate_part = jnp.dot(scaled, w_gate, preferred_element_type=jnp.float32)
    up_part = jnp.dot(scaled, w_up, preferred_element_type=jnp.float32)
    total_sq, gate_sum, up_sum = lax.psum((local_sq, gate_part, up_part), "cb")
    inv_in = lax.rsqrt(total_sq / width + EPS)[:, None]
    hidden = (jax.nn.silu(gate_sum * inv_in) * (up_sum * inv_in)).astype(jnp.bfloat16)
    partial_down = jnp.dot(hidden, w_down, preferred_element_type=jnp.float32)
    own_rows = tokens.shape[0] // lax.axis_size("ra")
    first_row = lax.axis_index("ra") * own_rows
    down = lax.psum_scatter(partial_down, "ra", scatter_dimension=0, tiled=True)
    residual = lax.dynamic_slice_in_dim(xfloat, first_row, own_rows, 0)
    mixed = 0.1 * residual + down
    out_sq = lax.psum(jnp.sum(mixed * mixed, axis=1), "cb")
    inv_out = lax.rsqrt(out_sq / width + EPS)[:, None]
    return (mixed * inv_out * out_gain.astype(jnp.float32)).astype(jnp.bfloat16)


def kernel(n_ra, width, subs, *refs):
    it = iter(refs)

    def take(count):
        return [next(it) for _ in range(count)]

    n = len(subs)
    tok_hbm, ng_hbm, wg_hbm, wu_hbm, wd_hbm, og_hbm, out_ref = take(7)
    tok, rest, ng, og, wgu, wd, xs, mixed, sqp, sqd, sqx, osq = take(12)
    xb, part, prec, xrec, hid, dn, yrec, zrec = [take(n) for _ in range(8)]
    ld, lw, s_d, r_d, s_x, r_x, s_h, r_h, s_y, r_y, s_z, r_z, s_o, r_o, s_q, r_q = take(16)
    depth, units = xs.shape[1], wd.shape[0]
    own = rest.shape[0]
    base = [sum(subs[:k]) for k in range(n)]
    nz = n_ra // 2
    ra, cb = lax.axis_index("ra"), lax.axis_index("cb")
    c, x = lax.rem(cb, 2), lax.div(cb, 2)
    y, z = lax.rem(ra, 2), lax.div(ra, 2)
    oc, ox, oy = 1 - c, 1 - x, 1 - y
    core_peer = (ra, x * 2 + oc)
    x_peer = (ra, ox * 2 + c)
    diag_peer = (ra, ox * 2 + oc)
    y_peer = (z * 2 + oy, cb)
    z_peers = [(lax.rem(z + d, nz) * 2 + y, cb) for d in range(1, nz)]
    mesh_id = pl.DeviceIdType.MESH
    pieces = column_pieces(2 * units)
    slices = [(i * depth // SLICES, depth // SLICES) for i in range(SLICES)]

    early = [
        pltpu.make_async_copy(tok_hbm, tok, ld.at[0]),
        pltpu.make_async_copy(ng_hbm, ng, ld.at[1]),
    ]
    weights = []
    for p, (start, size) in enumerate(pieces):
        got = []
        for i, (ref, low) in enumerate(((wg_hbm, 0), (wu_hbm, units))):
            lo, hi = max(start, low), min(start + size, low + units)
            if lo < hi:
                got.append(pltpu.make_async_copy(
                    ref.at[:, pl.ds(lo - low, hi - lo)], wgu.at[:, pl.ds(lo, hi - lo)], lw.at[p, i]))
        weights.append(got)
    late = [
        pltpu.make_async_copy(tok_hbm.at[pl.ds(pl.multiple_of(ra * own, own), own)], rest, ld.at[2]),
        pltpu.make_async_copy(og_hbm, og, ld.at[3]),
        pltpu.make_async_copy(wd_hbm, wd, ld.at[4]),
    ]
    for load in early + sum(weights, []) + late:
        load.start()

    barrier = pltpu.get_barrier_semaphore()
    peers = [core_peer, x_peer, diag_peer, y_peer] + z_peers
    for peer in peers:
        pl.semaphore_signal(barrier, inc=1, device_id=peer, device_id_type=mesh_id)

    sends = []

    def send(src, dst, s, r, peer):
        copy = pltpu.make_async_remote_copy(
            src_ref=src, dst_ref=dst, send_sem=s, recv_sem=r,
            device_id=peer, device_id_type=mesh_id)
        copy.start()
        sends.append(copy)
        return copy

    def project(k, p):
        with jax.named_scope(f"project{k}"):
            start, size = pieces[p]
            cols = pl.ds(start, size)
            got = jnp.dot(xb[k][...], wgu[:, cols], preferred_element_type=jnp.float32)
            part[k][:, :, :, cols] = got.reshape(2, 2, part[k].shape[2], size)

    def to_core(k, cols, p):
        return send(part[k].at[oc, :, :, cols], prec[k].at[:, :, cols], s_d.at[k, p], r_d.at[k, p], core_peer)

    def combine(k, copy, start, size, p):
        with jax.named_scope(f"combine{k}"):
            copy.wait_recv()
            cols = pl.ds(start, size)
            part[k][c, :, :, cols] += prec[k][:, :, cols]
            return send(part[k].at[c, ox, :, cols], xrec[k].at[:, cols], s_x.at[k, p], r_x.at[k, p], x_peer)

    def whole(k):
        for p in range(len(pieces)):
            project(k, p)
        return to_core(k, pl.ds(0, 2 * units), 0)

    def join(k, copy):
        return [combine(k, copy, 0, 2 * units, 0)]

    def activate(k, copies, inv):
        with jax.named_scope(f"activate{k}"):
            for copy in copies:
                copy.wait_recv()
            scale = inv[:part[k].shape[2], k:k + 1]
            gate = (part[k][c, x, :, :units] + xrec[k][:, :units]) * scale
            up = (part[k][c, x, :, units:] + xrec[k][:, units:]) * scale
            val = gate / (1.0 + jnp.exp(-gate)) * up
            hid[k][c, x] = val.astype(jnp.bfloat16).astype(jnp.float32)
            block = hid[k].at[c, x]
            hx = send(block, block, s_h.at[k, 0], r_h.at[k, 0], x_peer)
            h1 = send(block, block, s_h.at[k, 1], r_h.at[k, 1], core_peer)
            return hx, h1

    def forward(k, hx):
        with jax.named_scope(f"forward{k}"):
            hx.wait_recv()
            block = hid[k].at[c, ox]
            return send(block, block, s_h.at[k, 2], r_h.at[k, 2], core_peer)

    def arrived(k, h1, h2):
        h1.wait_recv()
        h2.wait_recv()

    def half(k, side):
        return hid[k][side].reshape(n_ra * subs[k] // 2, units).astype(jnp.bfloat16)

    def lower(k, h1, h2):
        with jax.named_scope(f"lower{k}"):
            pl.when(c != oy)(functools.partial(arrived, k, h1, h2))
            rows = half(k, oy)
            out = []
            for h, (start, size) in enumerate(slices):
                cols = pl.ds(start, size)
                got = jnp.dot(rows, wd[:, cols], preferred_element_type=jnp.float32)
                dn[k][oy, :, :, cols] = got.reshape(nz, subs[k], size)
                out.append(send(dn[k].at[oy, :, :, cols], yrec[k].at[:, :, cols],
                                s_y.at[k, h], r_y.at[k, h], y_peer))
            pl.when(c == oy)(functools.partial(arrived, k, h1, h2))
            got = jnp.dot(half(k, y), wd[...], preferred_element_type=jnp.float32)
            dn[k][y] = got.reshape(nz, subs[k], depth)
            return out

    def across(k, copies):
        with jax.named_scope(f"across{k}"):
            out = []
            for h, (start, size) in enumerate(slices):
                cols = pl.ds(start, size)
                copies[h].wait_recv()
                dn[k][y, :, :, cols] += yrec[k][:, :, cols]
                for d in range(1, nz):
                    out.append(send(
                        dn[k].at[y, lax.rem(z + d, nz), :, cols], zrec[k].at[d - 1, :, cols],
                        s_z.at[k, h, d - 1], r_z.at[k, h, d - 1], z_peers[d - 1]))
            return out

    def finish(k, copies):
        with jax.named_scope(f"finish{k}"):
            for copy in copies:
                copy.wait_recv()
            got = dn[k][y, z]
            for d in range(nz - 1):
                got = got + zrec[k][d]
            at = pl.ds(base[k], subs[k])
            got = mixed[at, :] + got
            mixed[at, :] = got
            osq[0, at, :] = jnp.broadcast_to(jnp.sum(got * got, axis=1, keepdims=True), (subs[k], LANES))
            return [
                send(osq.at[0, at], osq.at[i + 1, at], s_o.at[k, i], r_o.at[k, i], peer)
                for i, peer in enumerate((core_peer, x_peer, diag_peer))]

    def fill(k):
        xb[k][...] = jnp.concatenate(
            [xs[pl.ds((zz * 2 + yy) * own + base[k], subs[k]), :] for yy in range(2) for zz in range(nz)],
            axis=0).astype(jnp.bfloat16)

    def squares():
        with jax.named_scope("squares"):
            lane = lax.broadcasted_iota(jnp.int32, (own, LANES), 1)
            sqp[...] = jnp.zeros_like(sqp)
            for d in range(n_ra):
                xf = tok[pl.ds(d * own, own), :].astype(jnp.float32)
                sq = jnp.broadcast_to(jnp.sum(xf * xf, axis=1, keepdims=True), (own, LANES))
                for k in range(n):
                    at = ((d % 2) * nz + d // 2) * subs[k]
                    quarter = nz * subs[k] // 2
                    q, off = at // quarter, at % quarter
                    val = jnp.where(lane[:subs[k]] == k, sq[base[k]:base[k] + subs[k]], 0.0)
                    sqp[q // 2, q % 2, pl.ds(off, subs[k]), :] += val
            return send(sqp.at[oc], sqd, s_q.at[0], r_q.at[0], core_peer)

    with jax.named_scope("tokens"):
        for load in early:
            load.wait()
    with jax.named_scope("scale"):
        gain = ng[...].astype(jnp.float32).reshape(1, depth)
        for d in range(n_ra):
            at = pl.ds(d * own, own)
            xs[at, :] = tok[at, :].astype(jnp.float32) * gain
        fill(0)
    with jax.named_scope("enter"):
        pl.semaphore_wait(barrier, len(peers))

    a, b, h1, h2, hx, ys, zs, os = {}, {}, {}, {}, {}, {}, {}, {}
    b[0], b[1], waiting = [], [], []
    for k in range(2):
        for p, (start, size) in enumerate(pieces):
            if k == 0:
                with jax.named_scope("weights"):
                    for load in weights[p]:
                        load.wait()
            project(k, p)
            waiting.append((k, p, to_core(k, pl.ds(start, size), p)))
            if k == 0 and p == 0:
                q1 = squares()
            if len(waiting) > 1:
                kk, pp, copy = waiting.pop(0)
                b[kk].append(combine(kk, copy, *pieces[pp], pp))
            if k == 0 and p == 1:
                with jax.named_scope("share"):
                    q1.wait_recv()
                    sqp[c] += sqd[...]
                    q2 = send(sqp.at[c, ox], sqx, s_q.at[1], r_q.at[1], x_peer)
                fill(1)
    for kk, pp, copy in waiting:
        b[kk].append(combine(kk, copy, *pieces[pp], pp))
    for k in range(2, n):
        fill(k)
    for load in late:
        load.wait()
    mixed[...] = 0.1 * rest[...].astype(jnp.float32)
    for t in range(n + 3):
        if t + 2 < n:
            a[t + 2] = whole(t + 2)
        if t == 0:
            q2.wait_recv()
            inv = lax.rsqrt((sqp[c, x] + sqx[...]) / width + EPS)
        if t < n:
            hx[t], h1[t] = activate(t, b[t], inv)
        if t + 2 < n:
            b[t + 2] = join(t + 2, a[t + 2])
        if 0 <= t - 1 < n:
            h2[t - 1] = forward(t - 1, hx[t - 1])
        if t == n and n > 2:
            zs[n - 3] = across(n - 3, ys[n - 3])
        if 0 <= t - 1 < n:
            ys[t - 1] = lower(t - 1, h1[t - 1], h2[t - 1])
        if t == n and n > 3:
            os[n - 4] = finish(n - 4, zs[n - 4])
        if 0 <= t - 2 < n and t != n - 1:
            zs[t - 2] = across(t - 2, ys[t - 2])
        if 0 <= t - 3 < n and t != n - 1:
            os[t - 3] = finish(t - 3, zs[t - 3])
    with jax.named_scope("norm"):
        for k in range(n):
            for copy in os[k]:
                copy.wait_recv()
        osum = osq[0] + osq[1] + osq[2] + osq[3]
        inv_out = lax.rsqrt(osum / width + EPS)[:, :1]
        out_ref[...] = (mixed[...] * inv_out * og[...].astype(jnp.float32).reshape(1, depth)).astype(out_ref.dtype)
    with jax.named_scope("drain"):
        for copy in sends:
            copy.wait_send()


def column_pieces(total):
    tiles = total // TILE
    cuts = [tiles * i // PIECES * TILE for i in range(PIECES)] + [total]
    return [(lo, hi - lo) for lo, hi in zip(cuts[:-1], cuts[1:])]


def chunk_rows(own):
    unit = own // UNITS
    return [unit * share for share in SHARES]


def fused_body(n_ra, width, tokens, norm_gain, w_gate, w_up, w_down, out_gain):
    count, depth = tokens.shape
    units = w_down.shape[0]
    own = count // n_ra
    subs = chunk_rows(own)
    n, nz = len(subs), n_ra // 2
    f32, bf16 = jnp.float32, jnp.bfloat16
    dma = pltpu.SemaphoreType.DMA
    quarters = [n_ra * sub // 4 for sub in subs]
    most = max(quarters)
    return pl.pallas_call(
        functools.partial(kernel, n_ra, width, subs),
        out_shape=pltpu.VMEM((own, depth), bf16),
        in_specs=[pl.BlockSpec(memory_space=pl.ANY)] * 6,
        out_specs=pl.BlockSpec(memory_space=pltpu.VMEM),
        scratch_shapes=[
            pltpu.VMEM((count, depth), bf16),
            pltpu.VMEM((own, depth), bf16),
            pltpu.VMEM((depth,), bf16),
            pltpu.VMEM((depth,), bf16),
            pltpu.VMEM((depth, 2 * units), bf16),
            pltpu.VMEM((units, depth), bf16),
            pltpu.VMEM((count, depth), f32),
            pltpu.VMEM((own, depth), f32),
            pltpu.VMEM((2, 2, most, LANES), f32),
            pltpu.VMEM((2, most, LANES), f32),
            pltpu.VMEM((most, LANES), f32),
            pltpu.VMEM((4, own, LANES), f32),
            *[pltpu.VMEM((n_ra * sub, depth), bf16) for sub in subs],
            *[pltpu.VMEM((2, 2, quarter, 2 * units), f32) for quarter in quarters],
            *[pltpu.VMEM((2, quarter, 2 * units), f32) for quarter in quarters],
            *[pltpu.VMEM((quarter, 2 * units), f32) for quarter in quarters],
            *[pltpu.VMEM((2, 2, quarter, units), f32) for quarter in quarters],
            *[pltpu.VMEM((2, nz, sub, depth), f32) for sub in subs],
            *[pltpu.VMEM((nz, sub, depth), f32) for sub in subs],
            *[pltpu.VMEM((nz - 1, sub, depth), f32) for sub in subs],
            dma((5,)),
            dma((PIECES, 2)),
            *[dma((n, PIECES)) for _ in range(4)],
            *[dma((n, 3)) for _ in range(2)],
            *[dma((n, SLICES)) for _ in range(2)],
            *[dma((n, SLICES, nz - 1)) for _ in range(2)],
            *[dma((n, 3)) for _ in range(2)],
            *[dma((2,)) for _ in range(2)],
        ],
        compiler_params=pltpu.CompilerParams(
            collective_id=0, has_side_effects=True, vmem_limit_bytes=VMEM_BYTES),
    )(tokens, norm_gain, w_gate, w_up, w_down, out_gain)


def solution(mesh):
    n_ra, n_cb = mesh.shape["ra"], mesh.shape["cb"]

    def body(*args):
        tokens, w_down = args[0], args[4]
        count, depth = tokens.shape
        units = w_down.shape[0]
        width = depth * n_cb
        tiled = (
            n_cb == 4 and n_ra % 4 == 0 and n_ra > 2
            and count % (n_ra * UNITS * 8) == 0 and units % LANES == 0 and depth % TILE == 0
            and depth % (SLICES * LANES) == 0)
        if tiled:
            return fused_body(n_ra, width, *args)
        return plain_body(width, *args)

    return jax.shard_map(
        body,
        mesh=mesh,
        in_specs=(P(None, "cb"), P("cb"), P("cb", "ra"), P("cb", "ra"), P("ra", "cb"), P("cb")),
        out_specs=P("ra", "cb"),
        check_vma=False,
    )
```

```python
import functools

import jax
import jax.numpy as jnp
from jax import lax
from jax.experimental import pallas as pl
from jax.experimental.pallas import tpu as pltpu
from jax.sharding import PartitionSpec as P

EPS = 1e-06
LANES = 128
TILE = 256
WHOLE, OUTER, INNER = "whole", "outer", "inner"
CHUNKS = (
    (1, WHOLE), (2, WHOLE), (1, WHOLE), (1, WHOLE), (1, WHOLE), (1, OUTER), (1, INNER), (1, OUTER), (1, INNER))
UNITS = sum(share if owners == WHOLE else share / 2 for share, owners in CHUNKS)
FIRST_CUTS = (0, 1, 3, 5, 8)
SECOND_CUTS = (0, 3, 7)
VMEM_BYTES = 63 * 1024 * 1024 - 64 * 1024
STEPS = (
    "P2 A0 P3 P4", "J2 J3 A1 J4", "P5 F0 L0 A2", "J5 P6 Y0 A3", "J6 P7 F1 L1", "Z0 A4 J7 P8",
    "F2 L2 A5 J8", "Y1 F3 L3 A6", "Y2 F4 L4 A7", "F5 Y3 L5 A8", "Z1 F6 F7 Y4", "L6 F8 L7 Y5",
    "Z2 L8 Z3 Y6", "Y7 Z4 Y8 Z5", "Z6 Z7 Z8",
)
SLICES = (1, 1, 1, 1, 1, 2, 2, 2, 4)


def plain_body(width, tokens, norm_gain, w_gate, w_up, w_down, out_gain):
    xfloat = tokens.astype(jnp.float32)
    local_sq = jnp.sum(xfloat * xfloat, axis=1)
    scaled = (xfloat * norm_gain.astype(jnp.float32)).astype(jnp.bfloat16)
    gate_part = jnp.dot(scaled, w_gate, preferred_element_type=jnp.float32)
    up_part = jnp.dot(scaled, w_up, preferred_element_type=jnp.float32)
    total_sq, gate_sum, up_sum = lax.psum((local_sq, gate_part, up_part), "cb")
    inv_in = lax.rsqrt(total_sq / width + EPS)[:, None]
    hidden = (jax.nn.silu(gate_sum * inv_in) * (up_sum * inv_in)).astype(jnp.bfloat16)
    partial_down = jnp.dot(hidden, w_down, preferred_element_type=jnp.float32)
    own_rows = tokens.shape[0] // lax.axis_size("ra")
    first_row = lax.axis_index("ra") * own_rows
    down = lax.psum_scatter(partial_down, "ra", scatter_dimension=0, tiled=True)
    residual = lax.dynamic_slice_in_dim(xfloat, first_row, own_rows, 0)
    mixed = 0.1 * residual + down
    out_sq = lax.psum(jnp.sum(mixed * mixed, axis=1), "cb")
    inv_out = lax.rsqrt(out_sq / width + EPS)[:, None]
    return (mixed * inv_out * out_gain.astype(jnp.float32)).astype(jnp.bfloat16)


def column_pieces(k, total):
    cuts = FIRST_CUTS if k == 0 else SECOND_CUTS if k == 1 else (0,)
    edges = [cut * TILE for cut in cuts] + [total]
    return [(lo, hi - lo) for lo, hi in zip(edges[:-1], edges[1:])]


def chunk_layout(own, nz):
    zs = {WHOLE: list(range(nz)), OUTER: [0, nz - 1], INNER: list(range(1, nz - 1))}
    unit = own // int(UNITS)
    out, at = [], 0
    for share, owners in CHUNKS:
        out.append((at, unit * share, zs[owners]))
        at += unit * share if owners in (WHOLE, INNER) else 0
    return out


def semaphore_slots(total):
    n = len(CHUNKS)
    keys = ["rows", "rest", "gain", "out_gain", "down"]
    keys += [("weights", p) for p in range(len(FIRST_CUTS))]
    for k in range(n):
        keys += [("dr", k, p) for p in range(len(column_pieces(k, total)))]
        keys += [("xr", k), ("hr", k), ("fr", k), ("zr", k)] + [("yr", k, h) for h in range(SLICES[k])]
    keys += [("qr", 0), ("qr", 1), "or", "os"]
    for ring, depth in RINGS.items():
        keys += [(ring, i) for i in range(depth)]
    return {key: i for i, key in enumerate(keys)}


RINGS = {"ds": 3, "xs": 4, "hs": 4, "cs": 2, "fs": 2, "ys": 3, "zs": 3, "qs": 1}


def kernel(n_ra, width, layout, *refs):
    it = iter(refs)

    def take(count):
        return [next(it) for _ in range(count)]

    n = len(layout)
    tok_hbm, ng_hbm, wg_hbm, wu_hbm, wd_hbm, og_hbm, out_ref = take(7)
    first, tok, ng, og, wgu, wd, xs, mixed, sqp, sqd, sqx, osq = take(12)
    xb, part, prec, xrec, hid, dn, yrec, zrec = [take(n) for _ in range(8)]
    (sems,) = take(1)
    depth, units = xs.shape[1], wd.shape[0]
    own = mixed.shape[0]
    nz = n_ra // 2
    ra, cb = lax.axis_index("ra"), lax.axis_index("cb")
    c, x = lax.rem(cb, 2), lax.div(cb, 2)
    y, z = lax.rem(ra, 2), lax.div(ra, 2)
    oc, ox, oy = 1 - c, 1 - x, 1 - y
    core_peer = (ra, x * 2 + oc)
    x_peer = (ra, ox * 2 + c)
    diag_peer = (ra, ox * 2 + oc)
    y_peer = (z * 2 + oy, cb)
    mesh_id = pl.DeviceIdType.MESH
    slots = semaphore_slots(2 * units)
    head = layout[0][1]

    def sem(*key):
        return sems.at[slots[key if len(key) > 1 else key[0]]]

    early = [
        pltpu.make_async_copy(tok_hbm.at[pl.ds(d * own, head)], first.at[pl.ds(d * head, head)], sem("rows"))
        for d in range(n_ra)
    ] + [pltpu.make_async_copy(ng_hbm, ng, sem("gain"))]
    weights = []
    for p, (start, size) in enumerate(column_pieces(0, 2 * units)):
        got = []
        for ref, low in ((wg_hbm, 0), (wu_hbm, units)):
            lo, hi = max(start, low), min(start + size, low + units)
            if lo < hi:
                got.append(pltpu.make_async_copy(
                    ref.at[:, pl.ds(lo - low, hi - lo)], wgu.at[:, pl.ds(lo, hi - lo)], sem("weights", p)))
        weights.append(got)
    whole_tok = pltpu.make_async_copy(tok_hbm, tok, sem("rest"))
    late = [
        pltpu.make_async_copy(og_hbm, og, sem("out_gain")),
        pltpu.make_async_copy(wd_hbm, wd, sem("down")),
    ]
    for load in early + sum(weights[:3], []) + [whole_tok] + sum(weights[3:], []) + late:
        load.start()

    barrier = pltpu.get_barrier_semaphore()
    peers = [core_peer, x_peer, diag_peer, y_peer] + [(lax.rem(z + d, nz) * 2 + y, cb) for d in range(1, nz)]
    for peer in peers:
        pl.semaphore_signal(barrier, inc=1, device_id=peer, device_id_type=mesh_id)

    used = {ring: [None] * size for ring, size in RINGS.items()}
    turn = {ring: 0 for ring in RINGS}

    def slot_of(ring, leave):
        i = turn[ring] % RINGS[ring]
        turn[ring] += 1
        if used[ring][i] is not None:
            used[ring][i]()
        used[ring][i] = leave
        return sem(ring, i)

    def remote(src, dst, s, r, peer):
        return pltpu.make_async_remote_copy(
            src_ref=src, dst_ref=dst, send_sem=s, recv_sem=r, device_id=peer, device_id_type=mesh_id)

    def send(src, dst, ring, r, peer):
        made = []
        s = slot_of(ring, lambda: made[0].wait_send())
        made.append(remote(src, dst, s, r, peer))
        made[0].start()
        return made[0]

    def wait_bytes(ref, s):
        pltpu.make_async_copy(ref, ref, s).wait()

    def project(k, p=0):
        with jax.named_scope(f"project{k}"):
            start, size = column_pieces(k, 2 * units)[p]
            cols = pl.ds(start, size)
            got = jnp.dot(xb[k][...], wgu[:, cols], preferred_element_type=jnp.float32)
            part[k][:, :, :, cols] = got.reshape(2, 2, part[k].shape[2], size)

    def to_core(k, p=0):
        cols = pl.ds(*column_pieces(k, 2 * units)[p])
        return send(part[k].at[oc, :, :, cols], prec[k].at[:, :, cols], "ds", sem("dr", k, p), core_peer)

    leaving = {}

    def combine(k, p, copy):
        with jax.named_scope(f"combine{k}"):
            copy.wait_recv()
            cols = pl.ds(*column_pieces(k, 2 * units)[p])
            part[k][c, :, :, cols] += prec[k][:, :, cols]
            if k not in leaving:
                leaving[k] = slot_of("xs", lambda: wait_bytes(xrec[k], leaving[k]))
            remote(part[k].at[c, ox, :, cols], xrec[k].at[:, cols], leaving[k], sem("xr", k), x_peer).start()

    def activate(k, inv):
        with jax.named_scope(f"activate{k}"):
            wait_bytes(xrec[k], sem("xr", k))
            scale = inv[:part[k].shape[2], k:k + 1]
            gate = (part[k][c, x, :, :units] + xrec[k][:, :units]) * scale
            up = (part[k][c, x, :, units:] + xrec[k][:, units:]) * scale
            val = gate / (1.0 + jnp.exp(-gate)) * up
            hid[k][c, x] = val.astype(jnp.bfloat16).astype(jnp.float32)
            block = hid[k].at[c, x]
            hx = send(block, block, "hs", sem("hr", k), x_peer)
            send(block, block, "cs", sem("fr", k), core_peer)
            return hx

    def forward(k, hx):
        with jax.named_scope(f"forward{k}"):
            hx.wait_recv()
            block = hid[k].at[c, ox]
            send(block, block, "fs", sem("fr", k), core_peer)

    def lower(k):
        with jax.named_scope(f"lower{k}"):
            wait_bytes(hid[k].at[oc], sem("fr", k))
            _, sub, zs = layout[k]
            rows = hid[k][...].reshape(2 * len(zs) * sub, units).astype(jnp.bfloat16)
            s = slot_of("ys", lambda: wait_bytes(yrec[k], s))
            for h, (start, size) in enumerate(slices(k)):
                cols = pl.ds(start, size)
                got = jnp.dot(rows, wd[:, cols], preferred_element_type=jnp.float32)
                dn[k][:, :, :, cols] = got.reshape(2, len(zs), sub, size)
                remote(dn[k].at[oy, :, :, cols], yrec[k].at[:, :, cols], s, sem("yr", k, h), y_peer).start()

    def slices(k):
        return [(h * depth // SLICES[k], depth // SLICES[k]) for h in range(SLICES[k])]

    def owns(zs):
        return functools.reduce(jnp.logical_or, [z == zz for zz in zs])

    def across(k):
        with jax.named_scope(f"across{k}"):
            _, sub, zs = layout[k]

            def leave():
                if len(zs) == nz:
                    wait_bytes(zrec[k], s)
                else:
                    mine = owns(zs)
                    pl.when(mine)(lambda: wait_bytes(zrec[k].at[pl.ds(0, len(zs) - 1)], s))
                    pl.when(jnp.logical_not(mine))(lambda: wait_bytes(zrec[k].at[pl.ds(0, len(zs))], s))

            s = slot_of("zs", leave)
            for h, (start, size) in enumerate(slices(k)):
                cols = pl.ds(start, size)
                wait_bytes(yrec[k].at[:, :, cols], sem("yr", k, h))
                dn[k][y, :, :, cols] += yrec[k][:, :, cols]
                for j, zz in enumerate(zs):
                    @pl.when(z != zz)
                    def _(j=j, zz=zz, cols=cols):
                        slot = lax.rem(zz - z + nz, nz) - 1
                        remote(dn[k].at[y, j, :, cols], zrec[k].at[slot, :, cols], s, sem("zr", k),
                               (zz * 2 + y, cb)).start()

    def finish(k):
        base, sub, zs = layout[k]

        def run():
            wait_bytes(zrec[k], sem("zr", k))
            at = pl.ds(base, sub)
            index = z if len(zs) == nz else lax.div(z, nz - 1) if zs[0] == 0 else z - zs[0]
            got = dn[k][y, index]
            for d in range(nz - 1):
                got = got + zrec[k][d]
            got = mixed[at, :] + got
            mixed[at, :] = got
            osq[0, at, :] = jnp.broadcast_to(jnp.sum(got * got, axis=1, keepdims=True), (sub, LANES))
            for i, peer in enumerate((core_peer, x_peer, diag_peer)):
                remote(osq.at[0, at], osq.at[i + 1, at], sem("os"), sem("or"), peer).start()

        with jax.named_scope(f"finish{k}"):
            if len(zs) == nz:
                run()
            else:
                pl.when(owns(zs))(run)

    def fill(k):
        base, sub, zs = layout[k]
        xb[k][...] = jnp.concatenate(
            [xs[pl.ds((zz * 2 + yy) * own + base, sub), :] for yy in range(2) for zz in zs], axis=0).astype(jnp.bfloat16)

    def squares():
        with jax.named_scope("squares"):
            lane = lax.broadcasted_iota(jnp.int32, (own, LANES), 1)
            sqp[...] = jnp.zeros_like(sqp)
            for d in range(n_ra):
                xf = tok[pl.ds(d * own, own), :].astype(jnp.float32)
                sq = jnp.broadcast_to(jnp.sum(xf * xf, axis=1, keepdims=True), (own, LANES))
                for k, (base, sub, zs) in enumerate(layout):
                    if d // 2 not in zs:
                        continue
                    at = ((d % 2) * len(zs) + zs.index(d // 2)) * sub
                    quarter = len(zs) * sub // 2
                    q, off = at // quarter, at % quarter
                    val = jnp.where(lane[:sub] == k, sq[base:base + sub], 0.0)
                    sqp[q // 2, q % 2, pl.ds(off, sub), :] += val
            return send(sqp.at[oc], sqd, "qs", sem("qr", 0), core_peer)

    with jax.named_scope("tokens"):
        wait_bytes(first, sem("rows"))
        early[-1].wait()
    with jax.named_scope("scale"):
        gain = ng[...].astype(jnp.float32).reshape(1, depth)
        lead = first[...].astype(jnp.float32) * gain
        _, sub, zs = layout[0]
        xb[0][...] = jnp.concatenate(
            [lead[(zz * 2 + yy) * sub:(zz * 2 + yy + 1) * sub] for yy in range(2) for zz in zs], axis=0).astype(jnp.bfloat16)

    waiting = []

    def settle(left):
        while len(waiting) > left:
            k, p, copy = waiting.pop(0)
            combine(k, p, copy)

    for p, piece in enumerate(column_pieces(0, 2 * units)):
        with jax.named_scope("weights"):
            wait_bytes(wgu.at[:, pl.ds(*piece)], sem("weights", p))
        project(0, p)
        if p == 0:
            with jax.named_scope("enter"):
                pl.semaphore_wait(barrier, len(peers))
        waiting.append((0, p, to_core(0, p)))
        settle(2)
    with jax.named_scope("rest"):
        whole_tok.wait()
    q1 = squares()
    settle(1)
    with jax.named_scope("fill"):
        for d in range(n_ra):
            at = pl.ds(d * own, own)
            xs[at, :] = tok[at, :].astype(jnp.float32) * gain
        fill(1)
    settle(0)
    with jax.named_scope("share"):
        q1.wait_recv()
        sqp[c] += sqd[...]
        q2 = send(sqp.at[c, ox], sqx, "qs", sem("qr", 1), x_peer)
    for p in range(len(column_pieces(1, 2 * units))):
        project(1, p)
        waiting.append((1, p, to_core(1, p)))
        settle(1)
    settle(0)
    for k in range(2, n):
        fill(k)
    for load in late:
        load.wait()
    mixed[...] = 0.1 * tok[pl.ds(pl.multiple_of(ra * own, own), own), :].astype(jnp.float32)

    inv, sent, hx = None, {}, {}
    for step in [step for group in STEPS for step in group.split()]:
        what, k = step[0], int(step[1:])
        if what == "P":
            project(k)
            sent[k] = to_core(k)
        elif what == "J":
            combine(k, 0, sent[k])
        elif what == "A":
            if inv is None:
                q2.wait_recv()
                inv = lax.rsqrt((sqp[c, x] + sqx[...]) / width + EPS)
            hx[k] = activate(k, inv)
        elif what == "F":
            forward(k, hx[k])
        elif what == "L":
            lower(k)
        elif what == "Y":
            across(k)
        else:
            finish(k)
    with jax.named_scope("norm"):
        wait_bytes(osq.at[pl.ds(1, 3)], sem("or"))
        osum = osq[0] + osq[1] + osq[2] + osq[3]
        inv_out = lax.rsqrt(osum / width + EPS)[:, :1]
        out_ref[...] = (mixed[...] * inv_out * og[...].astype(jnp.float32).reshape(1, depth)).astype(out_ref.dtype)
    with jax.named_scope("drain"):
        for waits in used.values():
            for leave in waits:
                if leave is not None:
                    leave()
        wait_bytes(osq.at[pl.ds(1, 3)], sem("os"))


def fused_body(n_ra, width, tokens, norm_gain, w_gate, w_up, w_down, out_gain):
    count, depth = tokens.shape
    units = w_down.shape[0]
    own = count // n_ra
    nz = n_ra // 2
    layout = chunk_layout(own, nz)
    f32, bf16 = jnp.float32, jnp.bfloat16
    rows = [2 * len(zs) * sub for _, sub, zs in layout]
    quarters = [count // 4 for count in rows]
    most = max(quarters)
    return pl.pallas_call(
        functools.partial(kernel, n_ra, width, layout),
        out_shape=pltpu.VMEM((own, depth), bf16),
        in_specs=[pl.BlockSpec(memory_space=pl.ANY)] * 6,
        out_specs=pl.BlockSpec(memory_space=pltpu.VMEM),
        scratch_shapes=[
            pltpu.VMEM((rows[0], depth), bf16),
            pltpu.VMEM((count, depth), bf16),
            pltpu.VMEM((depth,), bf16),
            pltpu.VMEM((depth,), bf16),
            pltpu.VMEM((depth, 2 * units), bf16),
            pltpu.VMEM((units, depth), bf16),
            pltpu.VMEM((count, depth), f32),
            pltpu.VMEM((own, depth), f32),
            pltpu.VMEM((2, 2, most, LANES), f32),
            pltpu.VMEM((2, most, LANES), f32),
            pltpu.VMEM((most, LANES), f32),
            pltpu.VMEM((4, own, LANES), f32),
            *[pltpu.VMEM((count, depth), bf16) for count in rows],
            *[pltpu.VMEM((2, 2, quarter, 2 * units), f32) for quarter in quarters],
            *[pltpu.VMEM((2, quarter, 2 * units), f32) for quarter in quarters],
            *[pltpu.VMEM((quarter, 2 * units), f32) for quarter in quarters],
            *[pltpu.VMEM((2, 2, quarter, units), f32) for quarter in quarters],
            *[pltpu.VMEM((2, len(zs), sub, depth), f32) for _, sub, zs in layout],
            *[pltpu.VMEM((len(zs), sub, depth), f32) for _, sub, zs in layout],
            *[pltpu.VMEM((nz - 1, sub, depth), f32) for _, sub, _ in layout],
            pltpu.SemaphoreType.DMA((len(semaphore_slots(2 * units)),)),
        ],
        compiler_params=pltpu.CompilerParams(
            collective_id=0, has_side_effects=True, vmem_limit_bytes=VMEM_BYTES),
    )(tokens, norm_gain, w_gate, w_up, w_down, out_gain)


def solution(mesh):
    n_ra, n_cb = mesh.shape["ra"], mesh.shape["cb"]

    def body(*args):
        tokens, w_down = args[0], args[4]
        count, depth = tokens.shape
        units = w_down.shape[0]
        width = depth * n_cb
        tiled = (
            n_cb == 4 and n_ra == 8
            and count % (n_ra * int(UNITS) * 8) == 0 and units % LANES == 0 and depth % TILE == 0
            and depth % (max(SLICES) * LANES) == 0 and 2 * units > TILE * max(FIRST_CUTS + SECOND_CUTS))
        if tiled:
            return fused_body(n_ra, width, *args)
        return plain_body(width, *args)

    return jax.shard_map(
        body,
        mesh=mesh,
        in_specs=(P(None, "cb"), P("cb"), P("cb", "ra"), P("cb", "ra"), P("ra", "cb"), P("cb")),
        out_specs=P("ra", "cb"),
        check_vma=False,
    )
```

```python
import functools

import jax
import jax.numpy as jnp
from jax import lax
from jax.experimental import pallas as pl
from jax.experimental.pallas import tpu as pltpu
from jax.sharding import PartitionSpec as P

EPS = 1e-06
LANES = 128
TILE = 256
WHOLE, OUTER, INNER = "whole", "outer", "inner"
CHUNKS = (
    (1, WHOLE), (2, WHOLE), (1, WHOLE), (1, WHOLE), (1, WHOLE), (1, OUTER), (1, OUTER), (1, INNER), (1, INNER))
UNITS = sum(share if owners == WHOLE else share / 2 for share, owners in CHUNKS)
FIRST_CUTS = (0, 1, 3, 5, 8)
SECOND_CUTS = (0, 3, 7)
VMEM_BYTES = 63 * 1024 * 1024 - 64 * 1024
STEPS = (
    "P2 A0 P3 P4", "J2 J3 A1 J4", "P5 F0 L0 A2", "J5 P6 Y0 A3", "J6 P7 F1 L1", "Z0 A4 J7 P8",
    "F2 L2 A5 J8", "Y1 F3 L3 A6", "Y2 F4 L4 A7", "F5 Y3 L5 A8", "Z1 F6 F7 Y4", "L6 F8 L7 Y5",
    "Z2 L8 Z3 Y6", "Y7 Z4 Y8 Z5", "Z6 Z7 Z8",
)
SLICES = (1, 1, 1, 1, 1, 2, 2, 2, 2)


def plain_body(width, tokens, norm_gain, w_gate, w_up, w_down, out_gain):
    xfloat = tokens.astype(jnp.float32)
    local_sq = jnp.sum(xfloat * xfloat, axis=1)
    scaled = (xfloat * norm_gain.astype(jnp.float32)).astype(jnp.bfloat16)
    gate_part = jnp.dot(scaled, w_gate, preferred_element_type=jnp.float32)
    up_part = jnp.dot(scaled, w_up, preferred_element_type=jnp.float32)
    total_sq, gate_sum, up_sum = lax.psum((local_sq, gate_part, up_part), "cb")
    inv_in = lax.rsqrt(total_sq / width + EPS)[:, None]
    hidden = (jax.nn.silu(gate_sum * inv_in) * (up_sum * inv_in)).astype(jnp.bfloat16)
    partial_down = jnp.dot(hidden, w_down, preferred_element_type=jnp.float32)
    own_rows = tokens.shape[0] // lax.axis_size("ra")
    first_row = lax.axis_index("ra") * own_rows
    down = lax.psum_scatter(partial_down, "ra", scatter_dimension=0, tiled=True)
    residual = lax.dynamic_slice_in_dim(xfloat, first_row, own_rows, 0)
    mixed = 0.1 * residual + down
    out_sq = lax.psum(jnp.sum(mixed * mixed, axis=1), "cb")
    inv_out = lax.rsqrt(out_sq / width + EPS)[:, None]
    return (mixed * inv_out * out_gain.astype(jnp.float32)).astype(jnp.bfloat16)


def column_pieces(k, total):
    cuts = FIRST_CUTS if k == 0 else SECOND_CUTS if k == 1 else (0,)
    edges = [cut * TILE for cut in cuts] + [total]
    return [(lo, hi - lo) for lo, hi in zip(edges[:-1], edges[1:])]


def chunk_layout(own, nz):
    zs = {WHOLE: list(range(nz)), OUTER: [0, nz - 1], INNER: list(range(1, nz - 1))}
    unit = own // int(UNITS)
    out, at = [], [0] * nz
    for share, owners in CHUNKS:
        out.append((at[zs[owners][0]], unit * share, zs[owners]))
        for z in zs[owners]:
            at[z] += unit * share
    return out


def semaphore_slots(total):
    n = len(CHUNKS)
    keys = ["rows", "rest", "gain", "out_gain", "down"]
    keys += [("weights", p) for p in range(len(FIRST_CUTS))]
    for k in range(n):
        keys += [("dr", k, p) for p in range(len(column_pieces(k, total)))]
        keys += [("xr", k), ("hr", k), ("fr", k), ("zr", k)] + [("yr", k, h) for h in range(SLICES[k])]
    keys += [("qr", 0), ("qr", 1), "or", "os"]
    for ring, depth in RINGS.items():
        keys += [(ring, i) for i in range(depth)]
    return {key: i for i, key in enumerate(keys)}


RINGS = {"ds": 3, "xs": 4, "hs": 4, "cs": 2, "fs": 2, "ys": 3, "zs": 3, "qs": 1}


def kernel(n_ra, width, layout, *refs):
    it = iter(refs)

    def take(count):
        return [next(it) for _ in range(count)]

    n = len(layout)
    tok_hbm, ng_hbm, wg_hbm, wu_hbm, wd_hbm, og_hbm, out_ref = take(7)
    first, tok, ng, og, wgu, wd, xs, mixed, sqp, sqd, sqx, osq = take(12)
    xb, part, prec, xrec, hid, dn, yrec, zrec = [take(n) for _ in range(8)]
    (sems,) = take(1)
    depth, units = xs.shape[1], wd.shape[0]
    own = mixed.shape[0]
    nz = n_ra // 2
    ra, cb = lax.axis_index("ra"), lax.axis_index("cb")
    c, x = lax.rem(cb, 2), lax.div(cb, 2)
    y, z = lax.rem(ra, 2), lax.div(ra, 2)
    oc, ox, oy = 1 - c, 1 - x, 1 - y
    core_peer = (ra, x * 2 + oc)
    x_peer = (ra, ox * 2 + c)
    diag_peer = (ra, ox * 2 + oc)
    y_peer = (z * 2 + oy, cb)
    mesh_id = pl.DeviceIdType.MESH
    slots = semaphore_slots(2 * units)
    head = layout[0][1]

    def sem(*key):
        return sems.at[slots[key if len(key) > 1 else key[0]]]

    early = [
        pltpu.make_async_copy(tok_hbm.at[pl.ds(d * own, head)], first.at[pl.ds(d * head, head)], sem("rows"))
        for d in range(n_ra)
    ] + [pltpu.make_async_copy(ng_hbm, ng, sem("gain"))]
    weights = []
    for p, (start, size) in enumerate(column_pieces(0, 2 * units)):
        got = []
        for ref, low in ((wg_hbm, 0), (wu_hbm, units)):
            lo, hi = max(start, low), min(start + size, low + units)
            if lo < hi:
                got.append(pltpu.make_async_copy(
                    ref.at[:, pl.ds(lo - low, hi - lo)], wgu.at[:, pl.ds(lo, hi - lo)], sem("weights", p)))
        weights.append(got)
    whole_tok = pltpu.make_async_copy(tok_hbm, tok, sem("rest"))
    late = [
        pltpu.make_async_copy(og_hbm, og, sem("out_gain")),
        pltpu.make_async_copy(wd_hbm, wd, sem("down")),
    ]
    for load in early + sum(weights[:3], []) + [whole_tok] + sum(weights[3:], []) + late:
        load.start()

    barrier = pltpu.get_barrier_semaphore()
    peers = [core_peer, x_peer, diag_peer, y_peer] + [(lax.rem(z + d, nz) * 2 + y, cb) for d in range(1, nz)]
    for peer in peers:
        pl.semaphore_signal(barrier, inc=1, device_id=peer, device_id_type=mesh_id)

    used = {ring: [None] * size for ring, size in RINGS.items()}
    turn = {ring: 0 for ring in RINGS}

    def slot_of(ring, leave):
        i = turn[ring] % RINGS[ring]
        turn[ring] += 1
        if used[ring][i] is not None:
            used[ring][i]()
        used[ring][i] = leave
        return sem(ring, i)

    def remote(src, dst, s, r, peer):
        return pltpu.make_async_remote_copy(
            src_ref=src, dst_ref=dst, send_sem=s, recv_sem=r, device_id=peer, device_id_type=mesh_id)

    def send(src, dst, ring, r, peer):
        made = []
        s = slot_of(ring, lambda: made[0].wait_send())
        made.append(remote(src, dst, s, r, peer))
        made[0].start()
        return made[0]

    def wait_bytes(ref, s):
        pltpu.make_async_copy(ref, ref, s).wait()

    def project(k, p=0):
        with jax.named_scope(f"project{k}"):
            start, size = column_pieces(k, 2 * units)[p]
            cols = pl.ds(start, size)
            got = jnp.dot(xb[k][...], wgu[:, cols], preferred_element_type=jnp.float32)
            part[k][:, :, :, cols] = got.reshape(2, 2, part[k].shape[2], size)

    def to_core(k, p=0):
        cols = pl.ds(*column_pieces(k, 2 * units)[p])
        return send(part[k].at[oc, :, :, cols], prec[k].at[:, :, cols], "ds", sem("dr", k, p), core_peer)

    leaving = {}

    def combine(k, p, copy):
        with jax.named_scope(f"combine{k}"):
            copy.wait_recv()
            cols = pl.ds(*column_pieces(k, 2 * units)[p])
            part[k][c, :, :, cols] += prec[k][:, :, cols]
            if k not in leaving:
                leaving[k] = slot_of("xs", lambda: wait_bytes(xrec[k], leaving[k]))
            remote(part[k].at[c, ox, :, cols], xrec[k].at[:, cols], leaving[k], sem("xr", k), x_peer).start()

    def activate(k, inv):
        with jax.named_scope(f"activate{k}"):
            wait_bytes(xrec[k], sem("xr", k))
            scale = inv[:part[k].shape[2], k:k + 1]
            gate = (part[k][c, x, :, :units] + xrec[k][:, :units]) * scale
            up = (part[k][c, x, :, units:] + xrec[k][:, units:]) * scale
            val = gate / (1.0 + jnp.exp(-gate)) * up
            hid[k][c, x] = val.astype(jnp.bfloat16).astype(jnp.float32)
            block = hid[k].at[c, x]
            hx = send(block, block, "hs", sem("hr", k), x_peer)
            send(block, block, "cs", sem("fr", k), core_peer)
            return hx

    def forward(k, hx):
        with jax.named_scope(f"forward{k}"):
            hx.wait_recv()
            block = hid[k].at[c, ox]
            send(block, block, "fs", sem("fr", k), core_peer)

    def lower(k):
        with jax.named_scope(f"lower{k}"):
            wait_bytes(hid[k].at[oc], sem("fr", k))
            _, sub, zs = layout[k]
            rows = hid[k][...].reshape(2 * len(zs) * sub, units).astype(jnp.bfloat16)
            s = slot_of("ys", lambda: wait_bytes(yrec[k], s))
            for h, (start, size) in enumerate(slices(k)):
                cols = pl.ds(start, size)
                got = jnp.dot(rows, wd[:, cols], preferred_element_type=jnp.float32)
                dn[k][:, :, :, cols] = got.reshape(2, len(zs), sub, size)
                remote(dn[k].at[oy, :, :, cols], yrec[k].at[:, :, cols], s, sem("yr", k, h), y_peer).start()

    def slices(k):
        return [(h * depth // SLICES[k], depth // SLICES[k]) for h in range(SLICES[k])]

    def owns(zs):
        return functools.reduce(jnp.logical_or, [z == zz for zz in zs])

    def across(k):
        with jax.named_scope(f"across{k}"):
            _, sub, zs = layout[k]

            def leave():
                if len(zs) == nz:
                    wait_bytes(zrec[k], s)
                else:
                    mine = owns(zs)
                    pl.when(mine)(lambda: wait_bytes(zrec[k].at[pl.ds(0, len(zs) - 1)], s))
                    pl.when(jnp.logical_not(mine))(lambda: wait_bytes(zrec[k].at[pl.ds(0, len(zs))], s))

            s = slot_of("zs", leave)
            for h, (start, size) in enumerate(slices(k)):
                cols = pl.ds(start, size)
                wait_bytes(yrec[k].at[:, :, cols], sem("yr", k, h))
                dn[k][y, :, :, cols] += yrec[k][:, :, cols]
                for j, zz in enumerate(zs):
                    @pl.when(z != zz)
                    def _(j=j, zz=zz, cols=cols):
                        slot = lax.rem(zz - z + nz, nz) - 1
                        remote(dn[k].at[y, j, :, cols], zrec[k].at[slot, :, cols], s, sem("zr", k),
                               (zz * 2 + y, cb)).start()

    def finish(k):
        base, sub, zs = layout[k]

        def run():
            wait_bytes(zrec[k], sem("zr", k))
            at = pl.ds(base, sub)
            index = z if len(zs) == nz else lax.div(z, nz - 1) if zs[0] == 0 else z - zs[0]
            got = dn[k][y, index]
            for d in range(nz - 1):
                got = got + zrec[k][d]
            got = mixed[at, :] + got
            mixed[at, :] = got
            osq[0, at, :] = jnp.broadcast_to(jnp.sum(got * got, axis=1, keepdims=True), (sub, LANES))
            for i, peer in enumerate((core_peer, x_peer, diag_peer)):
                remote(osq.at[0, at], osq.at[i + 1, at], sem("os"), sem("or"), peer).start()

        with jax.named_scope(f"finish{k}"):
            if len(zs) == nz:
                run()
            else:
                pl.when(owns(zs))(run)

    def fill(k):
        base, sub, zs = layout[k]
        xb[k][...] = jnp.concatenate(
            [xs[pl.ds((zz * 2 + yy) * own + base, sub), :] for yy in range(2) for zz in zs], axis=0).astype(jnp.bfloat16)

    def squares():
        with jax.named_scope("squares"):
            lane = lax.broadcasted_iota(jnp.int32, (own, LANES), 1)
            sqp[...] = jnp.zeros_like(sqp)
            for d in range(n_ra):
                xf = tok[pl.ds(d * own, own), :].astype(jnp.float32)
                sq = jnp.broadcast_to(jnp.sum(xf * xf, axis=1, keepdims=True), (own, LANES))
                for k, (base, sub, zs) in enumerate(layout):
                    if d // 2 not in zs:
                        continue
                    at = ((d % 2) * len(zs) + zs.index(d // 2)) * sub
                    quarter = len(zs) * sub // 2
                    q, off = at // quarter, at % quarter
                    val = jnp.where(lane[:sub] == k, sq[base:base + sub], 0.0)
                    sqp[q // 2, q % 2, pl.ds(off, sub), :] += val
            return send(sqp.at[oc], sqd, "qs", sem("qr", 0), core_peer)

    with jax.named_scope("tokens"):
        wait_bytes(first, sem("rows"))
        early[-1].wait()
    with jax.named_scope("scale"):
        gain = ng[...].astype(jnp.float32).reshape(1, depth)
        lead = first[...].astype(jnp.float32) * gain
        _, sub, zs = layout[0]
        xb[0][...] = jnp.concatenate(
            [lead[(zz * 2 + yy) * sub:(zz * 2 + yy + 1) * sub] for yy in range(2) for zz in zs], axis=0).astype(jnp.bfloat16)

    waiting = []

    def settle(left):
        while len(waiting) > left:
            k, p, copy = waiting.pop(0)
            combine(k, p, copy)

    for p, piece in enumerate(column_pieces(0, 2 * units)):
        with jax.named_scope("weights"):
            wait_bytes(wgu.at[:, pl.ds(*piece)], sem("weights", p))
        project(0, p)
        if p == 0:
            with jax.named_scope("enter"):
                pl.semaphore_wait(barrier, len(peers))
        waiting.append((0, p, to_core(0, p)))
        settle(1 if p == 2 else 2)
    with jax.named_scope("rest"):
        whole_tok.wait()
    q1 = squares()
    settle(1)
    with jax.named_scope("fill"):
        for d in range(n_ra):
            at = pl.ds(d * own, own)
            xs[at, :] = tok[at, :].astype(jnp.float32) * gain
        fill(1)
    settle(0)
    with jax.named_scope("share"):
        q1.wait_recv()
        sqp[c] += sqd[...]
        q2 = send(sqp.at[c, ox], sqx, "qs", sem("qr", 1), x_peer)
    for p in range(len(column_pieces(1, 2 * units))):
        project(1, p)
        waiting.append((1, p, to_core(1, p)))
        settle(1)
    settle(0)
    for k in range(2, n):
        fill(k)
    for load in late:
        load.wait()
    mixed[...] = 0.1 * tok[pl.ds(pl.multiple_of(ra * own, own), own), :].astype(jnp.float32)

    inv, sent, hx = None, {}, {}
    for step in [step for group in STEPS for step in group.split()]:
        what, k = step[0], int(step[1:])
        if what == "P":
            project(k)
            sent[k] = to_core(k)
        elif what == "J":
            combine(k, 0, sent[k])
        elif what == "A":
            if inv is None:
                q2.wait_recv()
                inv = lax.rsqrt((sqp[c, x] + sqx[...]) / width + EPS)
            hx[k] = activate(k, inv)
        elif what == "F":
            forward(k, hx[k])
        elif what == "L":
            lower(k)
        elif what == "Y":
            across(k)
        else:
            finish(k)
    with jax.named_scope("norm"):
        wait_bytes(osq.at[pl.ds(1, 3)], sem("or"))
        osum = osq[0] + osq[1] + osq[2] + osq[3]
        inv_out = lax.rsqrt(osum / width + EPS)[:, :1]
        out_ref[...] = (mixed[...] * inv_out * og[...].astype(jnp.float32).reshape(1, depth)).astype(out_ref.dtype)
    with jax.named_scope("drain"):
        for waits in used.values():
            for leave in waits:
                if leave is not None:
                    leave()
        wait_bytes(osq.at[pl.ds(1, 3)], sem("os"))


def fused_body(n_ra, width, tokens, norm_gain, w_gate, w_up, w_down, out_gain):
    count, depth = tokens.shape
    units = w_down.shape[0]
    own = count // n_ra
    nz = n_ra // 2
    layout = chunk_layout(own, nz)
    f32, bf16 = jnp.float32, jnp.bfloat16
    rows = [2 * len(zs) * sub for _, sub, zs in layout]
    quarters = [count // 4 for count in rows]
    most = max(quarters)
    return pl.pallas_call(
        functools.partial(kernel, n_ra, width, layout),
        out_shape=pltpu.VMEM((own, depth), bf16),
        in_specs=[pl.BlockSpec(memory_space=pl.ANY)] * 6,
        out_specs=pl.BlockSpec(memory_space=pltpu.VMEM),
        scratch_shapes=[
            pltpu.VMEM((rows[0], depth), bf16),
            pltpu.VMEM((count, depth), bf16),
            pltpu.VMEM((depth,), bf16),
            pltpu.VMEM((depth,), bf16),
            pltpu.VMEM((depth, 2 * units), bf16),
            pltpu.VMEM((units, depth), bf16),
            pltpu.VMEM((count, depth), f32),
            pltpu.VMEM((own, depth), f32),
            pltpu.VMEM((2, 2, most, LANES), f32),
            pltpu.VMEM((2, most, LANES), f32),
            pltpu.VMEM((most, LANES), f32),
            pltpu.VMEM((4, own, LANES), f32),
            *[pltpu.VMEM((count, depth), bf16) for count in rows],
            *[pltpu.VMEM((2, 2, quarter, 2 * units), f32) for quarter in quarters],
            *[pltpu.VMEM((2, quarter, 2 * units), f32) for quarter in quarters],
            *[pltpu.VMEM((quarter, 2 * units), f32) for quarter in quarters],
            *[pltpu.VMEM((2, 2, quarter, units), f32) for quarter in quarters],
            *[pltpu.VMEM((2, len(zs), sub, depth), f32) for _, sub, zs in layout],
            *[pltpu.VMEM((len(zs), sub, depth), f32) for _, sub, zs in layout],
            *[pltpu.VMEM((nz - 1, sub, depth), f32) for _, sub, _ in layout],
            pltpu.SemaphoreType.DMA((len(semaphore_slots(2 * units)),)),
        ],
        compiler_params=pltpu.CompilerParams(
            collective_id=0, has_side_effects=True, vmem_limit_bytes=VMEM_BYTES),
    )(tokens, norm_gain, w_gate, w_up, w_down, out_gain)


def solution(mesh):
    n_ra, n_cb = mesh.shape["ra"], mesh.shape["cb"]

    def body(*args):
        tokens, w_down = args[0], args[4]
        count, depth = tokens.shape
        units = w_down.shape[0]
        width = depth * n_cb
        tiled = (
            n_cb == 4 and n_ra == 8
            and count % (n_ra * int(UNITS) * 8) == 0 and units % LANES == 0 and depth % TILE == 0
            and depth % (max(SLICES) * LANES) == 0 and 2 * units > TILE * max(FIRST_CUTS + SECOND_CUTS))
        if tiled:
            return fused_body(n_ra, width, *args)
        return plain_body(width, *args)

    return jax.shard_map(
        body,
        mesh=mesh,
        in_specs=(P(None, "cb"), P("cb"), P("cb", "ra"), P("cb", "ra"), P("ra", "cb"), P("cb")),
        out_specs=P("ra", "cb"),
        check_vma=False,
    )
```

```python
import functools

import jax
import jax.numpy as jnp
from jax import lax
from jax.experimental import pallas as pl
from jax.experimental.pallas import tpu as pltpu
from jax.sharding import PartitionSpec as P

EPS = 1e-06
LANES = 128
TILE = 256
WHOLE, OUTER, INNER = "whole", "outer", "inner"
CHUNKS = (
    (1, WHOLE), (2, WHOLE), (1, WHOLE), (1, WHOLE), (1, WHOLE), (1, OUTER), (1, OUTER), (1, INNER), (1, INNER))
UNITS = sum(share if owners == WHOLE else share / 2 for share, owners in CHUNKS)
FIRST_CUTS = (0, 1, 3, 5, 8)
SECOND_CUTS = (0, 3, 7)
HELD = (1, 0)
VMEM_BYTES = 63 * 1024 * 1024 - 64 * 1024
STEPS = (
    "P2 A0 P3 P4", "J2 J3 A1 J4", "P5 F0 L0 A2", "J5 P6 Y0 A3", "J6 P7 F1 L1", "Z0 A4 J7 P8",
    "F2 L2 A5 J8", "Y1 F3 L3 A6", "Y2 F4 L4 A7", "F5 Y3 L5 A8", "Z1 F6 F7 Y4", "L6 F8 L7 Y5",
    "Z2 L8 Z3 Y6", "Y7 Z4 Y8 Z5", "Z6 Z7 Z8",
)
SLICES = (1, 1, 1, 1, 1, 2, 2, 2, 2)


def plain_body(width, tokens, norm_gain, w_gate, w_up, w_down, out_gain):
    xfloat = tokens.astype(jnp.float32)
    local_sq = jnp.sum(xfloat * xfloat, axis=1)
    scaled = (xfloat * norm_gain.astype(jnp.float32)).astype(jnp.bfloat16)
    gate_part = jnp.dot(scaled, w_gate, preferred_element_type=jnp.float32)
    up_part = jnp.dot(scaled, w_up, preferred_element_type=jnp.float32)
    total_sq, gate_sum, up_sum = lax.psum((local_sq, gate_part, up_part), "cb")
    inv_in = lax.rsqrt(total_sq / width + EPS)[:, None]
    hidden = (jax.nn.silu(gate_sum * inv_in) * (up_sum * inv_in)).astype(jnp.bfloat16)
    partial_down = jnp.dot(hidden, w_down, preferred_element_type=jnp.float32)
    own_rows = tokens.shape[0] // lax.axis_size("ra")
    first_row = lax.axis_index("ra") * own_rows
    down = lax.psum_scatter(partial_down, "ra", scatter_dimension=0, tiled=True)
    residual = lax.dynamic_slice_in_dim(xfloat, first_row, own_rows, 0)
    mixed = 0.1 * residual + down
    out_sq = lax.psum(jnp.sum(mixed * mixed, axis=1), "cb")
    inv_out = lax.rsqrt(out_sq / width + EPS)[:, None]
    return (mixed * inv_out * out_gain.astype(jnp.float32)).astype(jnp.bfloat16)


def column_pieces(k, total):
    cuts = FIRST_CUTS if k == 0 else SECOND_CUTS if k == 1 else (0,)
    edges = [cut * TILE for cut in cuts] + [total]
    return [(lo, hi - lo) for lo, hi in zip(edges[:-1], edges[1:])]


def chunk_layout(own, nz):
    zs = {WHOLE: list(range(nz)), OUTER: [0, nz - 1], INNER: list(range(1, nz - 1))}
    unit = own // int(UNITS)
    out, at = [], [0] * nz
    for share, owners in CHUNKS:
        out.append((at[zs[owners][0]], unit * share, zs[owners]))
        for z in zs[owners]:
            at[z] += unit * share
    return out


def semaphore_slots(total):
    n = len(CHUNKS)
    done = ["rows", "rest", "gain", "out_gain", "down"]
    done += [("weights", p) for p in range(len(FIRST_CUTS))]
    done += [("dr", k, p) for k in range(2) for p in range(len(column_pieces(k, total)))]
    keys = done + [("dr", k, 0) for k in range(2, n)]
    for k in range(n):
        keys += [("xr", k), ("hr", k), ("fr", k), ("zr", k)] + [("yr", k, h) for h in range(SLICES[k])]
    keys += [("qr", 0), ("qr", 1), "or", "os"]
    keys += [(ring, i) for ring in ("ds", "xs", "qs") for i in range(RINGS[ring])]
    slots = {key: i for i, key in enumerate(key for key in keys if key not in REUSED)}
    later = [(ring, i) for ring in ("hs", "cs", "fs", "ys", "zs") for i in range(RINGS[ring])]
    slots.update({key: slots[taken] for key, taken in zip(later, done, strict=False)})
    for key, first in REUSED.items():
        slots[key] = slots[first]
    return slots


REUSED = {
    ("dr", 6, 0): ("dr", 2, 0), ("dr", 7, 0): ("dr", 3, 0), ("dr", 8, 0): ("dr", 4, 0),
    ("xr", 5): ("xr", 0), ("xr", 7): ("xr", 1), ("xr", 8): ("xr", 2),
    ("hr", 6): ("hr", 0), ("hr", 8): ("hr", 1),
    ("fr", 4): ("fr", 0), ("fr", 6): ("fr", 1), ("fr", 8): ("fr", 2),
    ("yr", 3, 0): ("yr", 0, 0), ("yr", 5, 0): ("yr", 1, 0), ("yr", 6, 0): ("yr", 2, 0), ("yr", 8, 0): ("yr", 3, 0),
    ("zr", 4): ("zr", 0),
}
RINGS = {"ds": 3, "xs": 4, "hs": 4, "cs": 2, "fs": 2, "ys": 3, "zs": 3, "qs": 1}


def kernel(n_ra, width, layout, *refs):
    it = iter(refs)

    def take(count):
        return [next(it) for _ in range(count)]

    n = len(layout)
    tok_hbm, ng_hbm, wg_hbm, wu_hbm, wd_hbm, og_hbm, out_ref = take(7)
    first, tok, ng, og, wgu, wd, xs, mixed, sqp, sqd, sqx, osq = take(12)
    xb, part, prec, xrec, hid, dn, yrec, zrec = [take(n) for _ in range(8)]
    (sems,) = take(1)
    depth, units = xs.shape[1], wd.shape[0]
    own = mixed.shape[0]
    nz = n_ra // 2
    ra, cb = lax.axis_index("ra"), lax.axis_index("cb")
    c, x = lax.rem(cb, 2), lax.div(cb, 2)
    y, z = lax.rem(ra, 2), lax.div(ra, 2)
    oc, ox, oy = 1 - c, 1 - x, 1 - y
    core_peer = (ra, x * 2 + oc)
    x_peer = (ra, ox * 2 + c)
    diag_peer = (ra, ox * 2 + oc)
    y_peer = (z * 2 + oy, cb)
    mesh_id = pl.DeviceIdType.MESH
    slots = semaphore_slots(2 * units)
    head = layout[0][1]

    def sem(*key):
        return sems.at[slots[key if len(key) > 1 else key[0]]]

    early = [
        pltpu.make_async_copy(tok_hbm.at[pl.ds(d * own, head)], first.at[pl.ds(d * head, head)], sem("rows"))
        for d in range(n_ra)
    ] + [pltpu.make_async_copy(ng_hbm, ng, sem("gain"))]
    weights = []
    for p, (start, size) in enumerate(column_pieces(0, 2 * units)):
        got = []
        for ref, low in ((wg_hbm, 0), (wu_hbm, units)):
            lo, hi = max(start, low), min(start + size, low + units)
            if lo < hi:
                got.append(pltpu.make_async_copy(
                    ref.at[:, pl.ds(lo - low, hi - lo)], wgu.at[:, pl.ds(lo, hi - lo)], sem("weights", p)))
        weights.append(got)
    whole_tok = pltpu.make_async_copy(tok_hbm, tok, sem("rest"))
    late = [
        pltpu.make_async_copy(og_hbm, og, sem("out_gain")),
        pltpu.make_async_copy(wd_hbm, wd, sem("down")),
    ]
    for load in early + sum(weights[:3], []) + [whole_tok] + sum(weights[3:], []) + late:
        load.start()

    barrier = pltpu.get_barrier_semaphore()
    peers = [core_peer, x_peer, diag_peer, y_peer] + [(lax.rem(z + d, nz) * 2 + y, cb) for d in range(1, nz)]
    for peer in peers:
        pl.semaphore_signal(barrier, inc=1, device_id=peer, device_id_type=mesh_id)

    used = {ring: [None] * size for ring, size in RINGS.items()}
    turn = {ring: 0 for ring in RINGS}

    def slot_of(ring, leave):
        i = turn[ring] % RINGS[ring]
        turn[ring] += 1
        if used[ring][i] is not None:
            used[ring][i]()
        used[ring][i] = leave
        return sem(ring, i)

    def remote(src, dst, s, r, peer):
        return pltpu.make_async_remote_copy(
            src_ref=src, dst_ref=dst, send_sem=s, recv_sem=r, device_id=peer, device_id_type=mesh_id)

    def send(src, dst, ring, r, peer):
        made = []
        s = slot_of(ring, lambda: made[0].wait_send())
        made.append(remote(src, dst, s, r, peer))
        made[0].start()
        return made[0]

    def wait_bytes(ref, s):
        pltpu.make_async_copy(ref, ref, s).wait()

    def project(k, p=0):
        with jax.named_scope(f"project{k}"):
            start, size = column_pieces(k, 2 * units)[p]
            cols = pl.ds(start, size)
            got = jnp.dot(xb[k][...], wgu[:, cols], preferred_element_type=jnp.float32)
            part[k][:, :, :, cols] = got.reshape(2, 2, part[k].shape[2], size)

    def to_core(k, p=0):
        cols = pl.ds(*column_pieces(k, 2 * units)[p])
        return send(part[k].at[oc, :, :, cols], prec[k].at[:, :, cols], "ds", sem("dr", k, p), core_peer)

    leaving, held = {}, []

    def combine(k, p, copy):
        with jax.named_scope(f"combine{k}"):
            copy.wait_recv()
            cols = pl.ds(*column_pieces(k, 2 * units)[p])
            part[k][c, :, :, cols] += prec[k][:, :, cols]
            if k not in leaving:
                leaving[k] = slot_of("xs", lambda: wait_bytes(xrec[k], leaving[k]))
            copy = remote(part[k].at[c, ox, :, cols], xrec[k].at[:, cols], leaving[k], sem("xr", k), x_peer)
            if (k, p) == HELD:
                pl.when(c == 0)(copy.start)
                held.append(copy)
            else:
                copy.start()

    def activate(k, inv):
        with jax.named_scope(f"activate{k}"):
            wait_bytes(xrec[k], sem("xr", k))
            scale = inv[:part[k].shape[2], k:k + 1]
            gate = (part[k][c, x, :, :units] + xrec[k][:, :units]) * scale
            up = (part[k][c, x, :, units:] + xrec[k][:, units:]) * scale
            val = gate / (1.0 + jnp.exp(-gate)) * up
            hid[k][c, x] = val.astype(jnp.bfloat16).astype(jnp.float32)
            block = hid[k].at[c, x]
            hx = send(block, block, "hs", sem("hr", k), x_peer)
            send(block, block, "cs", sem("fr", k), core_peer)
            return hx

    def forward(k, hx):
        with jax.named_scope(f"forward{k}"):
            hx.wait_recv()
            block = hid[k].at[c, ox]
            send(block, block, "fs", sem("fr", k), core_peer)

    def lower(k):
        with jax.named_scope(f"lower{k}"):
            wait_bytes(hid[k].at[oc], sem("fr", k))
            _, sub, zs = layout[k]
            rows = hid[k][...].reshape(2 * len(zs) * sub, units).astype(jnp.bfloat16)
            s = slot_of("ys", lambda: wait_bytes(yrec[k], s))
            for h, (start, size) in enumerate(slices(k)):
                cols = pl.ds(start, size)
                got = jnp.dot(rows, wd[:, cols], preferred_element_type=jnp.float32)
                dn[k][:, :, :, cols] = got.reshape(2, len(zs), sub, size)
                remote(dn[k].at[oy, :, :, cols], yrec[k].at[:, :, cols], s, sem("yr", k, h), y_peer).start()

    def slices(k):
        return [(h * depth // SLICES[k], depth // SLICES[k]) for h in range(SLICES[k])]

    def owns(zs):
        return functools.reduce(jnp.logical_or, [z == zz for zz in zs])

    def across(k):
        with jax.named_scope(f"across{k}"):
            _, sub, zs = layout[k]

            def leave():
                if len(zs) == nz:
                    wait_bytes(zrec[k], s)
                else:
                    mine = owns(zs)
                    pl.when(mine)(lambda: wait_bytes(zrec[k].at[pl.ds(0, len(zs) - 1)], s))
                    pl.when(jnp.logical_not(mine))(lambda: wait_bytes(zrec[k].at[pl.ds(0, len(zs))], s))

            s = slot_of("zs", leave)
            for h, (start, size) in enumerate(slices(k)):
                cols = pl.ds(start, size)
                wait_bytes(yrec[k].at[:, :, cols], sem("yr", k, h))
                dn[k][y, :, :, cols] += yrec[k][:, :, cols]
                for j, zz in enumerate(zs):
                    @pl.when(z != zz)
                    def _(j=j, zz=zz, cols=cols):
                        slot = lax.rem(zz - z + nz, nz) - 1
                        remote(dn[k].at[y, j, :, cols], zrec[k].at[slot, :, cols], s, sem("zr", k),
                               (zz * 2 + y, cb)).start()

    def finish(k):
        base, sub, zs = layout[k]

        def run():
            wait_bytes(zrec[k], sem("zr", k))
            at = pl.ds(base, sub)
            index = z if len(zs) == nz else lax.div(z, nz - 1) if zs[0] == 0 else z - zs[0]
            got = dn[k][y, index]
            for d in range(nz - 1):
                got = got + zrec[k][d]
            got = mixed[at, :] + got
            mixed[at, :] = got
            osq[0, at, :] = jnp.broadcast_to(jnp.sum(got * got, axis=1, keepdims=True), (sub, LANES))
            for i, peer in enumerate((core_peer, x_peer, diag_peer)):
                remote(osq.at[0, at], osq.at[i + 1, at], sem("os"), sem("or"), peer).start()

        with jax.named_scope(f"finish{k}"):
            if len(zs) == nz:
                run()
            else:
                pl.when(owns(zs))(run)

    def fill(k):
        base, sub, zs = layout[k]
        xb[k][...] = jnp.concatenate(
            [xs[pl.ds((zz * 2 + yy) * own + base, sub), :] for yy in range(2) for zz in zs], axis=0).astype(jnp.bfloat16)

    def squares():
        with jax.named_scope("squares"):
            lane = lax.broadcasted_iota(jnp.int32, (own, LANES), 1)
            sqp[...] = jnp.zeros_like(sqp)
            for d in range(n_ra):
                xf = tok[pl.ds(d * own, own), :].astype(jnp.float32)
                sq = jnp.broadcast_to(jnp.sum(xf * xf, axis=1, keepdims=True), (own, LANES))
                for k, (base, sub, zs) in enumerate(layout):
                    if d // 2 not in zs:
                        continue
                    at = ((d % 2) * len(zs) + zs.index(d // 2)) * sub
                    quarter = len(zs) * sub // 2
                    q, off = at // quarter, at % quarter
                    val = jnp.where(lane[:sub] == k, sq[base:base + sub], 0.0)
                    sqp[q // 2, q % 2, pl.ds(off, sub), :] += val
            return send(sqp.at[oc], sqd, "qs", sem("qr", 0), core_peer)

    with jax.named_scope("tokens"):
        wait_bytes(first, sem("rows"))
        early[-1].wait()
    with jax.named_scope("scale"):
        gain = ng[...].astype(jnp.float32).reshape(1, depth)
        lead = first[...].astype(jnp.float32) * gain
        _, sub, zs = layout[0]
        xb[0][...] = jnp.concatenate(
            [lead[(zz * 2 + yy) * sub:(zz * 2 + yy + 1) * sub] for yy in range(2) for zz in zs], axis=0).astype(jnp.bfloat16)

    waiting = []

    def settle(left):
        while len(waiting) > left:
            k, p, copy = waiting.pop(0)
            combine(k, p, copy)

    for p, piece in enumerate(column_pieces(0, 2 * units)):
        with jax.named_scope("weights"):
            wait_bytes(wgu.at[:, pl.ds(*piece)], sem("weights", p))
        project(0, p)
        if p == 0:
            with jax.named_scope("enter"):
                pl.semaphore_wait(barrier, len(peers))
        waiting.append((0, p, to_core(0, p)))
        settle(1 if p == 2 else 2)
    with jax.named_scope("rest"):
        whole_tok.wait()
    q1 = squares()
    settle(1)
    with jax.named_scope("fill"):
        for d in range(n_ra):
            at = pl.ds(d * own, own)
            xs[at, :] = tok[at, :].astype(jnp.float32) * gain
        fill(1)
    settle(0)
    with jax.named_scope("share"):
        q1.wait_recv()
        sqp[c] += sqd[...]
        q2 = send(sqp.at[c, ox], sqx, "qs", sem("qr", 1), x_peer)
    for p in range(len(column_pieces(1, 2 * units))):
        project(1, p)
        if held:
            pl.when(c != 0)(held.pop().start)
        waiting.append((1, p, to_core(1, p)))
        settle(1)
    settle(0)
    for k in range(2, n):
        fill(k)
    for load in late:
        load.wait()
    mixed[...] = 0.1 * tok[pl.ds(pl.multiple_of(ra * own, own), own), :].astype(jnp.float32)

    inv, sent, hx = None, {}, {}
    for step in [step for group in STEPS for step in group.split()]:
        what, k = step[0], int(step[1:])
        if what == "P":
            project(k)
            sent[k] = to_core(k)
        elif what == "J":
            combine(k, 0, sent[k])
        elif what == "A":
            if inv is None:
                q2.wait_recv()
                inv = lax.rsqrt((sqp[c, x] + sqx[...]) / width + EPS)
            hx[k] = activate(k, inv)
        elif what == "F":
            forward(k, hx[k])
        elif what == "L":
            lower(k)
        elif what == "Y":
            across(k)
        else:
            finish(k)
    with jax.named_scope("norm"):
        wait_bytes(osq.at[pl.ds(1, 3)], sem("or"))
        osum = osq[0] + osq[1] + osq[2] + osq[3]
        inv_out = lax.rsqrt(osum / width + EPS)[:, :1]
        out_ref[...] = (mixed[...] * inv_out * og[...].astype(jnp.float32).reshape(1, depth)).astype(out_ref.dtype)
    with jax.named_scope("drain"):
        for waits in used.values():
            for leave in waits:
                if leave is not None:
                    leave()
        wait_bytes(osq.at[pl.ds(1, 3)], sem("os"))


def fused_body(n_ra, width, tokens, norm_gain, w_gate, w_up, w_down, out_gain):
    count, depth = tokens.shape
    units = w_down.shape[0]
    own = count // n_ra
    nz = n_ra // 2
    layout = chunk_layout(own, nz)
    f32, bf16 = jnp.float32, jnp.bfloat16
    rows = [2 * len(zs) * sub for _, sub, zs in layout]
    quarters = [count // 4 for count in rows]
    most = max(quarters)
    return pl.pallas_call(
        functools.partial(kernel, n_ra, width, layout),
        out_shape=pltpu.VMEM((own, depth), bf16),
        in_specs=[pl.BlockSpec(memory_space=pl.ANY)] * 6,
        out_specs=pl.BlockSpec(memory_space=pltpu.VMEM),
        scratch_shapes=[
            pltpu.VMEM((rows[0], depth), bf16),
            pltpu.VMEM((count, depth), bf16),
            pltpu.VMEM((depth,), bf16),
            pltpu.VMEM((depth,), bf16),
            pltpu.VMEM((depth, 2 * units), bf16),
            pltpu.VMEM((units, depth), bf16),
            pltpu.VMEM((count, depth), f32),
            pltpu.VMEM((own, depth), f32),
            pltpu.VMEM((2, 2, most, LANES), f32),
            pltpu.VMEM((2, most, LANES), f32),
            pltpu.VMEM((most, LANES), f32),
            pltpu.VMEM((4, own, LANES), f32),
            *[pltpu.VMEM((count, depth), bf16) for count in rows],
            *[pltpu.VMEM((2, 2, quarter, 2 * units), f32) for quarter in quarters],
            *[pltpu.VMEM((2, quarter, 2 * units), f32) for quarter in quarters],
            *[pltpu.VMEM((quarter, 2 * units), f32) for quarter in quarters],
            *[pltpu.VMEM((2, 2, quarter, units), f32) for quarter in quarters],
            *[pltpu.VMEM((2, len(zs), sub, depth), f32) for _, sub, zs in layout],
            *[pltpu.VMEM((len(zs), sub, depth), f32) for _, sub, zs in layout],
            *[pltpu.VMEM((nz - 1, sub, depth), f32) for _, sub, _ in layout],
            pltpu.SemaphoreType.DMA((1 + max(semaphore_slots(2 * units).values()),)),
        ],
        compiler_params=pltpu.CompilerParams(
            collective_id=0, has_side_effects=True, vmem_limit_bytes=VMEM_BYTES),
    )(tokens, norm_gain, w_gate, w_up, w_down, out_gain)


def solution(mesh):
    n_ra, n_cb = mesh.shape["ra"], mesh.shape["cb"]

    def body(*args):
        tokens, w_down = args[0], args[4]
        count, depth = tokens.shape
        units = w_down.shape[0]
        width = depth * n_cb
        tiled = (
            n_cb == 4 and n_ra == 8
            and count % (n_ra * int(UNITS) * 8) == 0 and units % LANES == 0 and depth % TILE == 0
            and depth % (max(SLICES) * LANES) == 0 and 2 * units > TILE * max(FIRST_CUTS + SECOND_CUTS))
        if tiled:
            return fused_body(n_ra, width, *args)
        return plain_body(width, *args)

    return jax.shard_map(
        body,
        mesh=mesh,
        in_specs=(P(None, "cb"), P("cb"), P("cb", "ra"), P("cb", "ra"), P("ra", "cb"), P("cb")),
        out_specs=P("ra", "cb"),
        check_vma=False,
    )
```

```python
import functools

import jax
import jax.numpy as jnp
from jax import lax
from jax.experimental import pallas as pl
from jax.experimental.pallas import tpu as pltpu
from jax.sharding import PartitionSpec as P

EPS = 1e-06
LANES = 128
TILE = 256
WHOLE, OUTER, INNER = "whole", "outer", "inner"
CHUNKS = (
    (1, WHOLE), (2, WHOLE), (1, WHOLE), (1, WHOLE), (1, WHOLE), (1, OUTER), (1, OUTER), (1, INNER), (1, INNER))
UNITS = sum(share if owners == WHOLE else share / 2 for share, owners in CHUNKS)
FIRST_CUTS = (0, 1, 3, 5, 8)
SECOND_CUTS = (0, 3, 7)
HELD = (1, 0)
VMEM_BYTES = 63 * 1024 * 1024 - 64 * 1024
STEPS = (
    "P2 A0 P3 P4", "J2 J3 A1 J4", "P5 F0 L0 A2", "J5 P6 Y0 A3", "P7 F1 L1 Z0", "A4 J6 J7 P8",
    "F2 L2 A5 J8", "Y1 F3 L3 F4", "Y2 L4 A6 A7", "F5 Y3 L5 A8", "Z1 F6 F7 Y4", "L6 F8 L7 Y5",
    "Z2 L8 Z3 Y6", "Y7 Y8 Z4 Z5", "Z6 Z7 Z8",
)
SLICES = (1, 1, 1, 1, 1, 2, 2, 2, 2)


def plain_body(width, tokens, norm_gain, w_gate, w_up, w_down, out_gain):
    xfloat = tokens.astype(jnp.float32)
    local_sq = jnp.sum(xfloat * xfloat, axis=1)
    scaled = (xfloat * norm_gain.astype(jnp.float32)).astype(jnp.bfloat16)
    gate_part = jnp.dot(scaled, w_gate, preferred_element_type=jnp.float32)
    up_part = jnp.dot(scaled, w_up, preferred_element_type=jnp.float32)
    total_sq, gate_sum, up_sum = lax.psum((local_sq, gate_part, up_part), "cb")
    inv_in = lax.rsqrt(total_sq / width + EPS)[:, None]
    hidden = (jax.nn.silu(gate_sum * inv_in) * (up_sum * inv_in)).astype(jnp.bfloat16)
    partial_down = jnp.dot(hidden, w_down, preferred_element_type=jnp.float32)
    own_rows = tokens.shape[0] // lax.axis_size("ra")
    first_row = lax.axis_index("ra") * own_rows
    down = lax.psum_scatter(partial_down, "ra", scatter_dimension=0, tiled=True)
    residual = lax.dynamic_slice_in_dim(xfloat, first_row, own_rows, 0)
    mixed = 0.1 * residual + down
    out_sq = lax.psum(jnp.sum(mixed * mixed, axis=1), "cb")
    inv_out = lax.rsqrt(out_sq / width + EPS)[:, None]
    return (mixed * inv_out * out_gain.astype(jnp.float32)).astype(jnp.bfloat16)


def column_pieces(k, total):
    cuts = FIRST_CUTS if k == 0 else SECOND_CUTS if k == 1 else (0,)
    edges = [cut * TILE for cut in cuts] + [total]
    return [(lo, hi - lo) for lo, hi in zip(edges[:-1], edges[1:])]


def chunk_layout(own, nz):
    zs = {WHOLE: list(range(nz)), OUTER: [0, nz - 1], INNER: list(range(1, nz - 1))}
    unit = own // int(UNITS)
    out, at = [], [0] * nz
    for share, owners in CHUNKS:
        out.append((at[zs[owners][0]], unit * share, zs[owners]))
        for z in zs[owners]:
            at[z] += unit * share
    return out


def semaphore_slots(total):
    n = len(CHUNKS)
    done = ["rows", "rest", "gain", "out_gain", "down"]
    done += [("weights", p) for p in range(len(FIRST_CUTS))]
    done += [("dr", k, p) for k in range(2) for p in range(len(column_pieces(k, total)))]
    keys = done + [("dr", k, 0) for k in range(2, n)]
    for k in range(n):
        keys += [("xr", k), ("hr", k), ("fr", k), ("zr", k)] + [("yr", k, h) for h in range(SLICES[k])]
    keys += [("qr", 0), ("qr", 1), "or", "os"]
    keys += [(ring, i) for ring in ("ds", "xs", "qs") for i in range(RINGS[ring])]
    slots = {key: i for i, key in enumerate(key for key in keys if key not in REUSED)}
    later = [(ring, i) for ring in ("hs", "cs", "fs", "ys", "zs") for i in range(RINGS[ring])]
    slots.update({key: slots[taken] for key, taken in zip(later, done, strict=False)})
    for key, first in REUSED.items():
        slots[key] = slots[first]
    return slots


REUSED = {
    ("dr", 6, 0): ("dr", 2, 0), ("dr", 7, 0): ("dr", 3, 0), ("dr", 8, 0): ("dr", 4, 0),
    ("xr", 5): ("xr", 0), ("xr", 7): ("xr", 1), ("xr", 8): ("xr", 2),
    ("hr", 6): ("hr", 0), ("hr", 8): ("hr", 1),
    ("fr", 5): ("fr", 0), ("fr", 6): ("fr", 1), ("fr", 8): ("fr", 2),
    ("yr", 3, 0): ("yr", 0, 0), ("yr", 5, 0): ("yr", 1, 0), ("yr", 6, 0): ("yr", 2, 0), ("yr", 8, 0): ("yr", 3, 0),
    ("zr", 4): ("zr", 0),
}
RINGS = {"ds": 3, "xs": 4, "hs": 4, "cs": 2, "fs": 2, "ys": 3, "zs": 3, "qs": 1}


def kernel(n_ra, width, layout, *refs):
    it = iter(refs)

    def take(count):
        return [next(it) for _ in range(count)]

    n = len(layout)
    tok_hbm, ng_hbm, wg_hbm, wu_hbm, wd_hbm, og_hbm, out_ref = take(7)
    first, tok, ng, og, wgu, wd, xs, mixed, sqp, sqd, sqx, osq = take(12)
    xb, part, prec, xrec, hid, dn, yrec, zrec = [take(n) for _ in range(8)]
    (sems,) = take(1)
    depth, units = xs.shape[1], wd.shape[0]
    own = mixed.shape[0]
    nz = n_ra // 2
    ra, cb = lax.axis_index("ra"), lax.axis_index("cb")
    c, x = lax.rem(cb, 2), lax.div(cb, 2)
    y, z = lax.rem(ra, 2), lax.div(ra, 2)
    oc, ox, oy = 1 - c, 1 - x, 1 - y
    core_peer = (ra, x * 2 + oc)
    x_peer = (ra, ox * 2 + c)
    diag_peer = (ra, ox * 2 + oc)
    y_peer = (z * 2 + oy, cb)
    mesh_id = pl.DeviceIdType.MESH
    slots = semaphore_slots(2 * units)
    head = layout[0][1]

    def sem(*key):
        return sems.at[slots[key if len(key) > 1 else key[0]]]

    early = [
        pltpu.make_async_copy(tok_hbm.at[pl.ds(d * own, head)], first.at[pl.ds(d * head, head)], sem("rows"))
        for d in range(n_ra)
    ] + [pltpu.make_async_copy(ng_hbm, ng, sem("gain"))]
    weights = []
    for p, (start, size) in enumerate(column_pieces(0, 2 * units)):
        got = []
        for ref, low in ((wg_hbm, 0), (wu_hbm, units)):
            lo, hi = max(start, low), min(start + size, low + units)
            if lo < hi:
                got.append(pltpu.make_async_copy(
                    ref.at[:, pl.ds(lo - low, hi - lo)], wgu.at[:, pl.ds(lo, hi - lo)], sem("weights", p)))
        weights.append(got)
    whole_tok = pltpu.make_async_copy(tok_hbm, tok, sem("rest"))
    late = [
        pltpu.make_async_copy(og_hbm, og, sem("out_gain")),
        pltpu.make_async_copy(wd_hbm, wd, sem("down")),
    ]
    for load in early + sum(weights[:3], []) + [whole_tok] + sum(weights[3:], []) + late:
        load.start()

    barrier = pltpu.get_barrier_semaphore()
    peers = [core_peer, x_peer, diag_peer, y_peer] + [(lax.rem(z + d, nz) * 2 + y, cb) for d in range(1, nz)]
    for peer in peers:
        pl.semaphore_signal(barrier, inc=1, device_id=peer, device_id_type=mesh_id)

    used = {ring: [None] * size for ring, size in RINGS.items()}
    turn = {ring: 0 for ring in RINGS}

    def slot_of(ring, leave):
        i = turn[ring] % RINGS[ring]
        turn[ring] += 1
        if used[ring][i] is not None:
            used[ring][i]()
        used[ring][i] = leave
        return sem(ring, i)

    def remote(src, dst, s, r, peer):
        return pltpu.make_async_remote_copy(
            src_ref=src, dst_ref=dst, send_sem=s, recv_sem=r, device_id=peer, device_id_type=mesh_id)

    def send(src, dst, ring, r, peer):
        made = []
        s = slot_of(ring, lambda: made[0].wait_send())
        made.append(remote(src, dst, s, r, peer))
        made[0].start()
        return made[0]

    def wait_bytes(ref, s):
        pltpu.make_async_copy(ref, ref, s).wait()

    def project(k, p=0):
        with jax.named_scope(f"project{k}"):
            start, size = column_pieces(k, 2 * units)[p]
            cols = pl.ds(start, size)
            got = jnp.dot(xb[k][...], wgu[:, cols], preferred_element_type=jnp.float32)
            part[k][:, :, :, cols] = got.reshape(2, 2, part[k].shape[2], size)

    def to_core(k, p=0):
        cols = pl.ds(*column_pieces(k, 2 * units)[p])
        return send(part[k].at[oc, :, :, cols], prec[k].at[:, :, cols], "ds", sem("dr", k, p), core_peer)

    leaving, held = {}, []

    def combine(k, p, copy):
        with jax.named_scope(f"combine{k}"):
            copy.wait_recv()
            cols = pl.ds(*column_pieces(k, 2 * units)[p])
            part[k][c, :, :, cols] += prec[k][:, :, cols]
            if k not in leaving:
                leaving[k] = slot_of("xs", lambda: wait_bytes(xrec[k], leaving[k]))
            copy = remote(part[k].at[c, ox, :, cols], xrec[k].at[:, cols], leaving[k], sem("xr", k), x_peer)
            if (k, p) == HELD:
                pl.when(c == 0)(copy.start)
                held.append(copy)
            else:
                copy.start()

    def activate(k, inv):
        with jax.named_scope(f"activate{k}"):
            wait_bytes(xrec[k], sem("xr", k))
            scale = inv[:part[k].shape[2], k:k + 1]
            gate = (part[k][c, x, :, :units] + xrec[k][:, :units]) * scale
            up = (part[k][c, x, :, units:] + xrec[k][:, units:]) * scale
            val = gate / (1.0 + jnp.exp(-gate)) * up
            hid[k][c, x] = val.astype(jnp.bfloat16).astype(jnp.float32)
            block = hid[k].at[c, x]
            hx = send(block, block, "hs", sem("hr", k), x_peer)
            send(block, block, "cs", sem("fr", k), core_peer)
            return hx

    def forward(k, hx):
        with jax.named_scope(f"forward{k}"):
            hx.wait_recv()
            block = hid[k].at[c, ox]
            send(block, block, "fs", sem("fr", k), core_peer)

    def lower(k):
        with jax.named_scope(f"lower{k}"):
            wait_bytes(hid[k].at[oc], sem("fr", k))
            _, sub, zs = layout[k]
            rows = hid[k][...].reshape(2 * len(zs) * sub, units).astype(jnp.bfloat16)
            s = slot_of("ys", lambda: wait_bytes(yrec[k], s))
            for h, (start, size) in enumerate(slices(k)):
                cols = pl.ds(start, size)
                got = jnp.dot(rows, wd[:, cols], preferred_element_type=jnp.float32)
                dn[k][:, :, :, cols] = got.reshape(2, len(zs), sub, size)
                remote(dn[k].at[oy, :, :, cols], yrec[k].at[:, :, cols], s, sem("yr", k, h), y_peer).start()

    def slices(k):
        return [(h * depth // SLICES[k], depth // SLICES[k]) for h in range(SLICES[k])]

    def owns(zs):
        return functools.reduce(jnp.logical_or, [z == zz for zz in zs])

    def across(k):
        with jax.named_scope(f"across{k}"):
            _, sub, zs = layout[k]

            def leave():
                if len(zs) == nz:
                    wait_bytes(zrec[k], s)
                else:
                    mine = owns(zs)
                    pl.when(mine)(lambda: wait_bytes(zrec[k].at[pl.ds(0, len(zs) - 1)], s))
                    pl.when(jnp.logical_not(mine))(lambda: wait_bytes(zrec[k].at[pl.ds(0, len(zs))], s))

            s = slot_of("zs", leave)
            for h, (start, size) in enumerate(slices(k)):
                cols = pl.ds(start, size)
                wait_bytes(yrec[k].at[:, :, cols], sem("yr", k, h))
                dn[k][y, :, :, cols] += yrec[k][:, :, cols]
                for j, zz in enumerate(zs):
                    @pl.when(z != zz)
                    def _(j=j, zz=zz, cols=cols):
                        slot = lax.rem(zz - z + nz, nz) - 1
                        remote(dn[k].at[y, j, :, cols], zrec[k].at[slot, :, cols], s, sem("zr", k),
                               (zz * 2 + y, cb)).start()

    def finish(k):
        base, sub, zs = layout[k]

        def run():
            wait_bytes(zrec[k], sem("zr", k))
            at = pl.ds(base, sub)
            index = z if len(zs) == nz else lax.div(z, nz - 1) if zs[0] == 0 else z - zs[0]
            got = dn[k][y, index]
            for d in range(nz - 1):
                got = got + zrec[k][d]
            got = mixed[at, :] + got
            mixed[at, :] = got
            osq[0, at, :] = jnp.broadcast_to(jnp.sum(got * got, axis=1, keepdims=True), (sub, LANES))
            for i, peer in enumerate((core_peer, x_peer, diag_peer)):
                remote(osq.at[0, at], osq.at[i + 1, at], sem("os"), sem("or"), peer).start()

        with jax.named_scope(f"finish{k}"):
            if len(zs) == nz:
                run()
            else:
                pl.when(owns(zs))(run)

    def fill(k):
        base, sub, zs = layout[k]
        xb[k][...] = jnp.concatenate(
            [xs[pl.ds((zz * 2 + yy) * own + base, sub), :] for yy in range(2) for zz in zs], axis=0).astype(jnp.bfloat16)

    def squares():
        with jax.named_scope("squares"):
            lane = lax.broadcasted_iota(jnp.int32, (own, LANES), 1)
            sqp[...] = jnp.zeros_like(sqp)
            for d in range(n_ra):
                xf = tok[pl.ds(d * own, own), :].astype(jnp.float32)
                sq = jnp.broadcast_to(jnp.sum(xf * xf, axis=1, keepdims=True), (own, LANES))
                for k, (base, sub, zs) in enumerate(layout):
                    if d // 2 not in zs:
                        continue
                    at = ((d % 2) * len(zs) + zs.index(d // 2)) * sub
                    quarter = len(zs) * sub // 2
                    q, off = at // quarter, at % quarter
                    val = jnp.where(lane[:sub] == k, sq[base:base + sub], 0.0)
                    sqp[q // 2, q % 2, pl.ds(off, sub), :] += val
            return send(sqp.at[oc], sqd, "qs", sem("qr", 0), core_peer)

    with jax.named_scope("tokens"):
        wait_bytes(first, sem("rows"))
        early[-1].wait()
    with jax.named_scope("scale"):
        gain = ng[...].astype(jnp.float32).reshape(1, depth)
        lead = first[...].astype(jnp.float32) * gain
        _, sub, zs = layout[0]
        xb[0][...] = jnp.concatenate(
            [lead[(zz * 2 + yy) * sub:(zz * 2 + yy + 1) * sub] for yy in range(2) for zz in zs], axis=0).astype(jnp.bfloat16)

    waiting = []

    def settle(left):
        while len(waiting) > left:
            k, p, copy = waiting.pop(0)
            combine(k, p, copy)

    for p, piece in enumerate(column_pieces(0, 2 * units)):
        with jax.named_scope("weights"):
            wait_bytes(wgu.at[:, pl.ds(*piece)], sem("weights", p))
        project(0, p)
        if p == 0:
            with jax.named_scope("enter"):
                pl.semaphore_wait(barrier, len(peers))
        waiting.append((0, p, to_core(0, p)))
        settle(1 if p == 2 else 2)
    with jax.named_scope("rest"):
        whole_tok.wait()
    q1 = squares()
    settle(1)
    with jax.named_scope("fill"):
        for d in range(n_ra):
            at = pl.ds(d * own, own)
            xs[at, :] = tok[at, :].astype(jnp.float32) * gain
        fill(1)
    settle(0)
    with jax.named_scope("share"):
        q1.wait_recv()
        sqp[c] += sqd[...]
        q2 = send(sqp.at[c, ox], sqx, "qs", sem("qr", 1), x_peer)
    for p in range(len(column_pieces(1, 2 * units))):
        project(1, p)
        if held:
            pl.when(c != 0)(held.pop().start)
        waiting.append((1, p, to_core(1, p)))
        settle(1)
    settle(0)
    for k in range(2, n):
        fill(k)
    for load in late:
        load.wait()
    mixed[...] = 0.1 * tok[pl.ds(pl.multiple_of(ra * own, own), own), :].astype(jnp.float32)

    inv, sent, hx = None, {}, {}
    for step in [step for group in STEPS for step in group.split()]:
        what, k = step[0], int(step[1:])
        if what == "P":
            project(k)
            sent[k] = to_core(k)
        elif what == "J":
            combine(k, 0, sent[k])
        elif what == "A":
            if inv is None:
                q2.wait_recv()
                inv = lax.rsqrt((sqp[c, x] + sqx[...]) / width + EPS)
            hx[k] = activate(k, inv)
        elif what == "F":
            forward(k, hx[k])
        elif what == "L":
            lower(k)
        elif what == "Y":
            across(k)
        else:
            finish(k)
    with jax.named_scope("norm"):
        wait_bytes(osq.at[pl.ds(1, 3)], sem("or"))
        osum = osq[0] + osq[1] + osq[2] + osq[3]
        inv_out = lax.rsqrt(osum / width + EPS)[:, :1]
        out_ref[...] = (mixed[...] * inv_out * og[...].astype(jnp.float32).reshape(1, depth)).astype(out_ref.dtype)
    with jax.named_scope("drain"):
        for waits in used.values():
            for leave in waits:
                if leave is not None:
                    leave()
        wait_bytes(osq.at[pl.ds(1, 3)], sem("os"))


def fused_body(n_ra, width, tokens, norm_gain, w_gate, w_up, w_down, out_gain):
    count, depth = tokens.shape
    units = w_down.shape[0]
    own = count // n_ra
    nz = n_ra // 2
    layout = chunk_layout(own, nz)
    f32, bf16 = jnp.float32, jnp.bfloat16
    rows = [2 * len(zs) * sub for _, sub, zs in layout]
    quarters = [count // 4 for count in rows]
    most = max(quarters)
    return pl.pallas_call(
        functools.partial(kernel, n_ra, width, layout),
        out_shape=pltpu.VMEM((own, depth), bf16),
        in_specs=[pl.BlockSpec(memory_space=pl.ANY)] * 6,
        out_specs=pl.BlockSpec(memory_space=pltpu.VMEM),
        scratch_shapes=[
            pltpu.VMEM((rows[0], depth), bf16),
            pltpu.VMEM((count, depth), bf16),
            pltpu.VMEM((depth,), bf16),
            pltpu.VMEM((depth,), bf16),
            pltpu.VMEM((depth, 2 * units), bf16),
            pltpu.VMEM((units, depth), bf16),
            pltpu.VMEM((count, depth), f32),
            pltpu.VMEM((own, depth), f32),
            pltpu.VMEM((2, 2, most, LANES), f32),
            pltpu.VMEM((2, most, LANES), f32),
            pltpu.VMEM((most, LANES), f32),
            pltpu.VMEM((4, own, LANES), f32),
            *[pltpu.VMEM((count, depth), bf16) for count in rows],
            *[pltpu.VMEM((2, 2, quarter, 2 * units), f32) for quarter in quarters],
            *[pltpu.VMEM((2, quarter, 2 * units), f32) for quarter in quarters],
            *[pltpu.VMEM((quarter, 2 * units), f32) for quarter in quarters],
            *[pltpu.VMEM((2, 2, quarter, units), f32) for quarter in quarters],
            *[pltpu.VMEM((2, len(zs), sub, depth), f32) for _, sub, zs in layout],
            *[pltpu.VMEM((len(zs), sub, depth), f32) for _, sub, zs in layout],
            *[pltpu.VMEM((nz - 1, sub, depth), f32) for _, sub, _ in layout],
            pltpu.SemaphoreType.DMA((1 + max(semaphore_slots(2 * units).values()),)),
        ],
        compiler_params=pltpu.CompilerParams(
            collective_id=0, has_side_effects=True, vmem_limit_bytes=VMEM_BYTES),
    )(tokens, norm_gain, w_gate, w_up, w_down, out_gain)


def solution(mesh):
    n_ra, n_cb = mesh.shape["ra"], mesh.shape["cb"]

    def body(*args):
        tokens, w_down = args[0], args[4]
        count, depth = tokens.shape
        units = w_down.shape[0]
        width = depth * n_cb
        tiled = (
            n_cb == 4 and n_ra == 8
            and count % (n_ra * int(UNITS) * 8) == 0 and units % LANES == 0 and depth % TILE == 0
            and depth % (max(SLICES) * LANES) == 0 and 2 * units > TILE * max(FIRST_CUTS + SECOND_CUTS))
        if tiled:
            return fused_body(n_ra, width, *args)
        return plain_body(width, *args)

    return jax.shard_map(
        body,
        mesh=mesh,
        in_specs=(P(None, "cb"), P("cb"), P("cb", "ra"), P("cb", "ra"), P("ra", "cb"), P("cb")),
        out_specs=P("ra", "cb"),
        check_vma=False,
    )
```

```python
import functools

import jax
import jax.numpy as jnp
from jax import lax
from jax.experimental import pallas as pl
from jax.experimental.pallas import tpu as pltpu
from jax.sharding import PartitionSpec as P

EPS = 1e-06
LANES = 128
TILE = 256
WHOLE, OUTER, INNER = "whole", "outer", "inner"
CHUNKS = (
    (1, WHOLE), (2, WHOLE), (1, WHOLE), (1, WHOLE), (1, WHOLE), (1, OUTER), (1, OUTER), (1, INNER), (1, INNER))
UNITS = sum(share if owners == WHOLE else share / 2 for share, owners in CHUNKS)
FIRST_CUTS = (0, 1, 3, 5, 8)
SECOND_CUTS = (0, 3, 7)
HELD = (1, 0)
VMEM_BYTES = 63 * 1024 * 1024 - 64 * 1024
STEPS = (
    "P2 A0 P3 P4", "J2 J3 A1 J4", "P5 F0 L0 A2", "J5 P6 Y0 A3", "P7 F1 L1 Z0", "A4 J6 J7 P8",
    "F2 L2 A5 J8", "Y1 F3 L3 F4", "Y2 L4 A6 A7", "F5 Y3 L5 A8", "Z1 F6 F7 Y4", "L6 F8 L7 Y5",
    "Z2 L8 Z3 Y6", "Y7 Y8 Z4 Z5", "Z6 Z7 Z8",
)
SLICES = (1, 1, 1, 1, 1, 2, 2, 2, 2)


def plain_body(width, tokens, norm_gain, w_gate, w_up, w_down, out_gain):
    xfloat = tokens.astype(jnp.float32)
    local_sq = jnp.sum(xfloat * xfloat, axis=1)
    scaled = (xfloat * norm_gain.astype(jnp.float32)).astype(jnp.bfloat16)
    gate_part = jnp.dot(scaled, w_gate, preferred_element_type=jnp.float32)
    up_part = jnp.dot(scaled, w_up, preferred_element_type=jnp.float32)
    total_sq, gate_sum, up_sum = lax.psum((local_sq, gate_part, up_part), "cb")
    inv_in = lax.rsqrt(total_sq / width + EPS)[:, None]
    hidden = (jax.nn.silu(gate_sum * inv_in) * (up_sum * inv_in)).astype(jnp.bfloat16)
    partial_down = jnp.dot(hidden, w_down, preferred_element_type=jnp.float32)
    own_rows = tokens.shape[0] // lax.axis_size("ra")
    first_row = lax.axis_index("ra") * own_rows
    down = lax.psum_scatter(partial_down, "ra", scatter_dimension=0, tiled=True)
    residual = lax.dynamic_slice_in_dim(xfloat, first_row, own_rows, 0)
    mixed = 0.1 * residual + down
    out_sq = lax.psum(jnp.sum(mixed * mixed, axis=1), "cb")
    inv_out = lax.rsqrt(out_sq / width + EPS)[:, None]
    return (mixed * inv_out * out_gain.astype(jnp.float32)).astype(jnp.bfloat16)


def column_pieces(k, total):
    cuts = FIRST_CUTS if k == 0 else SECOND_CUTS if k == 1 else (0,)
    edges = [cut * TILE for cut in cuts] + [total]
    return [(lo, hi - lo) for lo, hi in zip(edges[:-1], edges[1:])]


def chunk_layout(own, nz):
    zs = {WHOLE: list(range(nz)), OUTER: [0, nz - 1], INNER: list(range(1, nz - 1))}
    unit = own // int(UNITS)
    out, at = [], [0] * nz
    for share, owners in CHUNKS:
        out.append((at[zs[owners][0]], unit * share, zs[owners]))
        for z in zs[owners]:
            at[z] += unit * share
    return out


def semaphore_slots(total):
    n = len(CHUNKS)
    done = ["rows", "rest", "gain", "out_gain", "down"]
    done += [("weights", p) for p in range(len(FIRST_CUTS))]
    done += [("dr", k, p) for k in range(2) for p in range(len(column_pieces(k, total)))]
    keys = done + [("dr", k, 0) for k in range(2, n)]
    for k in range(n):
        keys += [("xr", k), ("hr", k), ("fr", k), ("zr", k)] + [("yr", k, h) for h in range(SLICES[k])]
    keys += [("qr", 0), ("qr", 1), "or", "os"]
    keys += [(ring, i) for ring in ("ds", "xs", "qs") for i in range(RINGS[ring])]
    slots = {key: i for i, key in enumerate(key for key in keys if key not in REUSED)}
    later = [(ring, i) for ring in ("hs", "cs", "fs", "ys", "zs") for i in range(RINGS[ring])]
    slots.update({key: slots[taken] for key, taken in zip(later, done, strict=False)})
    for key, first in REUSED.items():
        slots[key] = slots[first]
    return slots


REUSED = {
    ("dr", 6, 0): ("dr", 2, 0), ("dr", 7, 0): ("dr", 3, 0), ("dr", 8, 0): ("dr", 4, 0),
    ("xr", 5): ("xr", 0), ("xr", 7): ("xr", 1), ("xr", 8): ("xr", 2),
    ("hr", 6): ("hr", 0), ("hr", 8): ("hr", 1),
    ("fr", 5): ("fr", 0), ("fr", 6): ("fr", 1), ("fr", 8): ("fr", 2),
    ("yr", 3, 0): ("yr", 0, 0), ("yr", 5, 0): ("yr", 1, 0), ("yr", 6, 0): ("yr", 2, 0), ("yr", 8, 0): ("yr", 3, 0),
    ("zr", 4): ("zr", 0),
}
RINGS = {"ds": 3, "xs": 4, "hs": 4, "cs": 2, "fs": 2, "ys": 3, "zs": 3, "qs": 1}


def kernel(n_ra, width, layout, *refs):
    it = iter(refs)

    def take(count):
        return [next(it) for _ in range(count)]

    n = len(layout)
    tok_hbm, ng_hbm, wg_hbm, wu_hbm, wd_hbm, og_hbm, out_ref = take(7)
    first, tok, ng, og, wgu, wd, xs, mixed, sqp, sqd, sqx, osq = take(12)
    xb, part, prec, xrec, hid, dn, yrec, zrec = [take(n) for _ in range(8)]
    (sems,) = take(1)
    depth, units = xs.shape[1], wd.shape[0]
    own = mixed.shape[0]
    nz = n_ra // 2
    ra, cb = lax.axis_index("ra"), lax.axis_index("cb")
    c, x = lax.rem(cb, 2), lax.div(cb, 2)
    y, z = lax.rem(ra, 2), lax.div(ra, 2)
    oc, ox, oy = 1 - c, 1 - x, 1 - y
    core_peer = (ra, x * 2 + oc)
    x_peer = (ra, ox * 2 + c)
    diag_peer = (ra, ox * 2 + oc)
    y_peer = (z * 2 + oy, cb)
    mesh_id = pl.DeviceIdType.MESH
    slots = semaphore_slots(2 * units)
    head = layout[0][1]

    def sem(*key):
        return sems.at[slots[key if len(key) > 1 else key[0]]]

    early = [
        pltpu.make_async_copy(tok_hbm.at[pl.ds(d * own, head)], first.at[pl.ds(d * head, head)], sem("rows"))
        for d in range(n_ra)
    ] + [pltpu.make_async_copy(ng_hbm, ng, sem("gain"))]
    weights = []
    for p, (start, size) in enumerate(column_pieces(0, 2 * units)):
        got = []
        for ref, low in ((wg_hbm, 0), (wu_hbm, units)):
            lo, hi = max(start, low), min(start + size, low + units)
            if lo < hi:
                got.append(pltpu.make_async_copy(
                    ref.at[:, pl.ds(lo - low, hi - lo)], wgu.at[:, pl.ds(lo, hi - lo)], sem("weights", p)))
        weights.append(got)
    whole_tok = pltpu.make_async_copy(tok_hbm, tok, sem("rest"))
    late = [
        pltpu.make_async_copy(og_hbm, og, sem("out_gain")),
        pltpu.make_async_copy(wd_hbm, wd, sem("down")),
    ]
    for load in early + sum(weights[:3], []) + [whole_tok] + sum(weights[3:], []) + late:
        load.start()

    barrier = pltpu.get_barrier_semaphore()
    peers = [core_peer, x_peer, diag_peer, y_peer] + [(lax.rem(z + d, nz) * 2 + y, cb) for d in range(1, nz)]
    for peer in peers:
        pl.semaphore_signal(barrier, inc=1, device_id=peer, device_id_type=mesh_id)

    used = {ring: [None] * size for ring, size in RINGS.items()}
    turn = {ring: 0 for ring in RINGS}

    def slot_of(ring, leave):
        i = turn[ring] % RINGS[ring]
        turn[ring] += 1
        if used[ring][i] is not None:
            used[ring][i]()
        used[ring][i] = leave
        return sem(ring, i)

    def remote(src, dst, s, r, peer):
        return pltpu.make_async_remote_copy(
            src_ref=src, dst_ref=dst, send_sem=s, recv_sem=r, device_id=peer, device_id_type=mesh_id)

    def send(src, dst, ring, r, peer):
        made = []
        s = slot_of(ring, lambda: made[0].wait_send())
        made.append(remote(src, dst, s, r, peer))
        made[0].start()
        return made[0]

    def wait_bytes(ref, s):
        pltpu.make_async_copy(ref, ref, s).wait()

    def project(k, p=0):
        with jax.named_scope(f"project{k}"):
            start, size = column_pieces(k, 2 * units)[p]
            cols = pl.ds(start, size)
            got = jnp.dot(xb[k][...], wgu[:, cols], preferred_element_type=jnp.float32)
            part[k][:, :, :, cols] = got.reshape(2, 2, part[k].shape[2], size)

    def to_core(k, p=0):
        cols = pl.ds(*column_pieces(k, 2 * units)[p])
        return send(part[k].at[oc, :, :, cols], prec[k].at[:, :, cols], "ds", sem("dr", k, p), core_peer)

    leaving, held = {}, []

    def combine(k, p, copy):
        with jax.named_scope(f"combine{k}"):
            copy.wait_recv()
            cols = pl.ds(*column_pieces(k, 2 * units)[p])
            part[k][c, :, :, cols] += prec[k][:, :, cols]
            if k not in leaving:
                leaving[k] = slot_of("xs", lambda: wait_bytes(xrec[k], leaving[k]))
            copy = remote(part[k].at[c, ox, :, cols], xrec[k].at[:, cols], leaving[k], sem("xr", k), x_peer)
            if (k, p) == HELD:
                pl.when(c == 0)(copy.start)
                held.append(copy)
            else:
                copy.start()

    def activate(k, inv):
        with jax.named_scope(f"activate{k}"):
            wait_bytes(xrec[k], sem("xr", k))
            scale = inv[:part[k].shape[2], k:k + 1]
            gate = (part[k][c, x, :, :units] + xrec[k][:, :units]) * scale
            up = (part[k][c, x, :, units:] + xrec[k][:, units:]) * scale
            val = gate / (1.0 + jnp.exp(-gate)) * up
            hid[k][c, x] = val.astype(jnp.bfloat16).astype(jnp.float32)
            block = hid[k].at[c, x]
            hx = send(block, block, "hs", sem("hr", k), x_peer)
            send(block, block, "cs", sem("fr", k), core_peer)
            return hx

    def forward(k, hx):
        with jax.named_scope(f"forward{k}"):
            hx.wait_recv()
            block = hid[k].at[c, ox]
            send(block, block, "fs", sem("fr", k), core_peer)

    def lower(k):
        with jax.named_scope(f"lower{k}"):
            wait_bytes(hid[k].at[oc], sem("fr", k))
            _, sub, zs = layout[k]
            rows = hid[k][...].reshape(2 * len(zs) * sub, units).astype(jnp.bfloat16)
            s = slot_of("ys", lambda: wait_bytes(yrec[k], s))
            for h, (start, size) in enumerate(slices(k)):
                cols = pl.ds(start, size)
                got = jnp.dot(rows, wd[:, cols], preferred_element_type=jnp.float32)
                dn[k][:, :, :, cols] = got.reshape(2, len(zs), sub, size)
                remote(dn[k].at[oy, :, :, cols], yrec[k].at[:, :, cols], s, sem("yr", k, h), y_peer).start()

    def slices(k):
        return [(h * depth // SLICES[k], depth // SLICES[k]) for h in range(SLICES[k])]

    def owns(zs):
        return functools.reduce(jnp.logical_or, [z == zz for zz in zs])

    def across(k):
        with jax.named_scope(f"across{k}"):
            _, sub, zs = layout[k]

            def leave():
                if len(zs) == nz:
                    wait_bytes(zrec[k], s)
                else:
                    mine = owns(zs)
                    pl.when(mine)(lambda: wait_bytes(zrec[k].at[pl.ds(0, len(zs) - 1)], s))
                    pl.when(jnp.logical_not(mine))(lambda: wait_bytes(zrec[k].at[pl.ds(0, len(zs))], s))

            s = slot_of("zs", leave)
            for h, (start, size) in enumerate(slices(k)):
                cols = pl.ds(start, size)
                wait_bytes(yrec[k].at[:, :, cols], sem("yr", k, h))
                dn[k][y, :, :, cols] += yrec[k][:, :, cols]
                for j, zz in enumerate(zs):
                    @pl.when(z != zz)
                    def _(j=j, zz=zz, cols=cols):
                        slot = lax.rem(zz - z + nz, nz) - 1
                        remote(dn[k].at[y, j, :, cols], zrec[k].at[slot, :, cols], s, sem("zr", k),
                               (zz * 2 + y, cb)).start()

    def finish(k):
        base, sub, zs = layout[k]

        def run():
            wait_bytes(zrec[k], sem("zr", k))
            at = pl.ds(base, sub)
            index = z if len(zs) == nz else lax.div(z, nz - 1) if zs[0] == 0 else z - zs[0]
            got = dn[k][y, index]
            for d in range(nz - 1):
                got = got + zrec[k][d]
            got = mixed[at, :] + got
            mixed[at, :] = got
            osq[0, at, :] = jnp.broadcast_to(jnp.sum(got * got, axis=1, keepdims=True), (sub, LANES))
            for i, peer in enumerate((core_peer, x_peer, diag_peer)):
                remote(osq.at[0, at], osq.at[i + 1, at], sem("os"), sem("or"), peer).start()

        with jax.named_scope(f"finish{k}"):
            if len(zs) == nz:
                run()
            else:
                pl.when(owns(zs))(run)

    def fill(k):
        base, sub, zs = layout[k]
        xb[k][...] = jnp.concatenate(
            [xs[pl.ds((zz * 2 + yy) * own + base, sub), :] for yy in range(2) for zz in zs], axis=0).astype(jnp.bfloat16)

    def squares():
        with jax.named_scope("squares"):
            lane = lax.broadcasted_iota(jnp.int32, (own, LANES), 1)
            sqp[...] = jnp.zeros_like(sqp)
            for d in range(n_ra):
                xf = tok[pl.ds(d * own, own), :].astype(jnp.float32)
                sq = jnp.broadcast_to(jnp.sum(xf * xf, axis=1, keepdims=True), (own, LANES))
                for k, (base, sub, zs) in enumerate(layout):
                    if d // 2 not in zs:
                        continue
                    at = ((d % 2) * len(zs) + zs.index(d // 2)) * sub
                    quarter = len(zs) * sub // 2
                    q, off = at // quarter, at % quarter
                    val = jnp.where(lane[:sub] == k, sq[base:base + sub], 0.0)
                    sqp[q // 2, q % 2, pl.ds(off, sub), :] += val
            return send(sqp.at[oc], sqd, "qs", sem("qr", 0), core_peer)

    with jax.named_scope("tokens"):
        wait_bytes(first, sem("rows"))
        early[-1].wait()
    with jax.named_scope("scale"):
        gain = ng[...].astype(jnp.float32).reshape(1, depth)
        lead = first[...].astype(jnp.float32) * gain
        _, sub, zs = layout[0]
        xb[0][...] = jnp.concatenate(
            [lead[(zz * 2 + yy) * sub:(zz * 2 + yy + 1) * sub] for yy in range(2) for zz in zs], axis=0).astype(jnp.bfloat16)

    waiting = []

    def settle(left):
        while len(waiting) > left:
            k, p, copy = waiting.pop(0)
            combine(k, p, copy)

    for p, piece in enumerate(column_pieces(0, 2 * units)):
        with jax.named_scope("weights"):
            wait_bytes(wgu.at[:, pl.ds(*piece)], sem("weights", p))
        project(0, p)
        if p == 0:
            with jax.named_scope("enter"):
                pl.semaphore_wait(barrier, len(peers))
        waiting.append((0, p, to_core(0, p)))
        settle(1 if p in (2, 3) else 2)
    with jax.named_scope("rest"):
        whole_tok.wait()
    q1 = squares()
    settle(1)
    with jax.named_scope("fill"):
        for d in range(n_ra):
            at = pl.ds(d * own, own)
            xs[at, :] = tok[at, :].astype(jnp.float32) * gain
        fill(1)
    for p in range(len(column_pieces(1, 2 * units))):
        project(1, p)
        if held:
            pl.when(c != 0)(held.pop().start)
        waiting.append((1, p, to_core(1, p)))
        if p == 1:
            with jax.named_scope("share"):
                q1.wait_recv()
                sqp[c] += sqd[...]
                q2 = send(sqp.at[c, ox], sqx, "qs", sem("qr", 1), x_peer)
        settle(1)
    settle(0)
    for k in range(2, n):
        fill(k)
    for load in late:
        load.wait()
    mixed[...] = 0.1 * tok[pl.ds(pl.multiple_of(ra * own, own), own), :].astype(jnp.float32)

    inv, sent, hx = None, {}, {}
    for step in [step for group in STEPS for step in group.split()]:
        what, k = step[0], int(step[1:])
        if what == "P":
            project(k)
            sent[k] = to_core(k)
        elif what == "J":
            combine(k, 0, sent[k])
        elif what == "A":
            if inv is None:
                q2.wait_recv()
                inv = lax.rsqrt((sqp[c, x] + sqx[...]) / width + EPS)
            hx[k] = activate(k, inv)
        elif what == "F":
            forward(k, hx[k])
        elif what == "L":
            lower(k)
        elif what == "Y":
            across(k)
        else:
            finish(k)
    with jax.named_scope("norm"):
        wait_bytes(osq.at[pl.ds(1, 3)], sem("or"))
        osum = osq[0] + osq[1] + osq[2] + osq[3]
        inv_out = lax.rsqrt(osum / width + EPS)[:, :1]
        out_ref[...] = (mixed[...] * inv_out * og[...].astype(jnp.float32).reshape(1, depth)).astype(out_ref.dtype)
    with jax.named_scope("drain"):
        for waits in used.values():
            for leave in waits:
                if leave is not None:
                    leave()
        wait_bytes(osq.at[pl.ds(1, 3)], sem("os"))


def fused_body(n_ra, width, tokens, norm_gain, w_gate, w_up, w_down, out_gain):
    count, depth = tokens.shape
    units = w_down.shape[0]
    own = count // n_ra
    nz = n_ra // 2
    layout = chunk_layout(own, nz)
    f32, bf16 = jnp.float32, jnp.bfloat16
    rows = [2 * len(zs) * sub for _, sub, zs in layout]
    quarters = [count // 4 for count in rows]
    most = max(quarters)
    return pl.pallas_call(
        functools.partial(kernel, n_ra, width, layout),
        out_shape=pltpu.VMEM((own, depth), bf16),
        in_specs=[pl.BlockSpec(memory_space=pl.ANY)] * 6,
        out_specs=pl.BlockSpec(memory_space=pltpu.VMEM),
        scratch_shapes=[
            pltpu.VMEM((rows[0], depth), bf16),
            pltpu.VMEM((count, depth), bf16),
            pltpu.VMEM((depth,), bf16),
            pltpu.VMEM((depth,), bf16),
            pltpu.VMEM((depth, 2 * units), bf16),
            pltpu.VMEM((units, depth), bf16),
            pltpu.VMEM((count, depth), f32),
            pltpu.VMEM((own, depth), f32),
            pltpu.VMEM((2, 2, most, LANES), f32),
            pltpu.VMEM((2, most, LANES), f32),
            pltpu.VMEM((most, LANES), f32),
            pltpu.VMEM((4, own, LANES), f32),
            *[pltpu.VMEM((count, depth), bf16) for count in rows],
            *[pltpu.VMEM((2, 2, quarter, 2 * units), f32) for quarter in quarters],
            *[pltpu.VMEM((2, quarter, 2 * units), f32) for quarter in quarters],
            *[pltpu.VMEM((quarter, 2 * units), f32) for quarter in quarters],
            *[pltpu.VMEM((2, 2, quarter, units), f32) for quarter in quarters],
            *[pltpu.VMEM((2, len(zs), sub, depth), f32) for _, sub, zs in layout],
            *[pltpu.VMEM((len(zs), sub, depth), f32) for _, sub, zs in layout],
            *[pltpu.VMEM((nz - 1, sub, depth), f32) for _, sub, _ in layout],
            pltpu.SemaphoreType.DMA((1 + max(semaphore_slots(2 * units).values()),)),
        ],
        compiler_params=pltpu.CompilerParams(
            collective_id=0, has_side_effects=True, vmem_limit_bytes=VMEM_BYTES),
    )(tokens, norm_gain, w_gate, w_up, w_down, out_gain)


def solution(mesh):
    n_ra, n_cb = mesh.shape["ra"], mesh.shape["cb"]

    def body(*args):
        tokens, w_down = args[0], args[4]
        count, depth = tokens.shape
        units = w_down.shape[0]
        width = depth * n_cb
        tiled = (
            n_cb == 4 and n_ra == 8
            and count % (n_ra * int(UNITS) * 8) == 0 and units % LANES == 0 and depth % TILE == 0
            and depth % (max(SLICES) * LANES) == 0 and 2 * units > TILE * max(FIRST_CUTS + SECOND_CUTS))
        if tiled:
            return fused_body(n_ra, width, *args)
        return plain_body(width, *args)

    return jax.shard_map(
        body,
        mesh=mesh,
        in_specs=(P(None, "cb"), P("cb"), P("cb", "ra"), P("cb", "ra"), P("ra", "cb"), P("cb")),
        out_specs=P("ra", "cb"),
        check_vma=False,
    )
```
